512 devices in a mesh: fs: 64 (over z, y), tp: 8 (over x, core).
Axes of the slice: x: 4, y: 8, z: 8, core: 2. Of those that a mesh axis runs over, the one named last changes fastest.
Arguments:
- layer_input: bfloat16 [65536, 2048], P('fs'), may hold values from -6 to 6
- value_cotangent: bfloat16 [65536, 1024], P('fs', 'tp'), may hold values from -0.0234375 to 0.0234375
- mixed_output: bfloat16 [65536, 1024], P('fs'), may hold values from -6 to 6
- output_cotangent: bfloat16 [65536, 2048], P('fs', 'tp'), may hold values from -0.0234375 to 0.0234375
- value_weight: float32 [2048, 1024], P('fs', 'tp'), may hold values from -0.125 to 0.125
- out_weight: float32 [1024, 2048], P('fs', 'tp'), may hold values from -0.1875 to 0.1875
- value_basis: bfloat16 [2048, 256], P('fs'), may hold values from -0.125 to 0.125
- out_basis: bfloat16 [1024, 256], P('fs'), may hold values from -0.1875 to 0.1875
- value_first: float32 [256, 1024], P('fs', 'tp'), may hold values from -6 to 6
- value_second: float32 [256, 1024], P('fs', 'tp'), may hold values from 0.5 to 2
- out_first: float32 [256, 2048], P('fs', 'tp'), may hold values from -6 to 6
- out_second: float32 [256, 2048], P('fs', 'tp'), may hold values from 0.5 to 2
Outputs:
- value_new: float32 [2048, 1024], P('fs', 'tp')
- out_new: float32 [1024, 2048], P('fs', 'tp')
- value_step: float32 [2048, 1024], P('fs', 'tp')
- out_step: float32 [1024, 2048], P('fs', 'tp')
- value_copy: bfloat16 [2048, 1024], P(None, 'tp')
- out_copy: bfloat16 [1024, 2048], P(None, 'tp')
- value_first_new: float32 [256, 1024], P('fs', 'tp')
- value_second_new: float32 [256, 1024], P('fs', 'tp')
- out_first_new: float32 [256, 2048], P('fs', 'tp')
- out_second_new: float32 [256, 2048], P('fs', 'tp')
The draws below stay inside these ranges and needn't reach their ends.
All inputs are finite; a program needn't handle non-finite values.
Results may differ from the reference program's by a relative error of at most 0.00045.
Values may be sent and summed in bfloat16 or wider, within the bound.
No kernel may reach another device: no remote copies, remote signals or barrier semaphores. Data moves between devices by JAX's collectives and lax.ppermute only.
A program may use at most 64 MiB of HBM per device.

```python
import math
import jax
import jax.numpy as jnp
from jax import lax

D = 2048
W = 1024
R = 256
TOKENS = 65536


def levels(stream_key, dims, cuts, low, largest):
    gain = 1.0
    for axis_at, shards_of in cuts:
        steps = jax.random.uniform(jax.random.fold_in(jax.random.fold_in(stream_key, 6), axis_at), (shards_of,), jnp.float32, low / len(cuts), largest / len(cuts))
        gain = gain * jnp.repeat(jnp.exp(steps), dims[axis_at] // shards_of).reshape((-1,) + (1,) * (len(dims) - 1 - axis_at))
    return gain


def noise(stream_key, shape, spread, reach, split=(), kind=jnp.bfloat16):
    entries = jax.random.normal(stream_key, shape, jnp.float32) * spread
    if len(split) > 0:
        entries = levels(stream_key, shape, split, -0.22, 0.18) * entries
    return jnp.clip(entries, min=-reach, max=reach).astype(kind)


def setup_inputs(seed: int = 0) -> dict:
    key_of = jax.random.split(jax.random.key(seed), 13)
    return {
        "layer_input": noise(key_of[0], (TOKENS, D), 1.0, 6.0, ((0, 64),)),
        "value_cotangent": noise(key_of[1], (TOKENS, W), (1.0 / TOKENS ** 0.5), 0.0234375, ((0, 64), (1, 8))),
        "mixed_output": noise(key_of[2], (TOKENS, W), 1.0, 6.0, ((0, 64),)),
        "output_cotangent": noise(key_of[3], (TOKENS, D), (1.0 / TOKENS ** 0.5), 0.0234375, ((0, 64), (1, 8))),
        "value_weight": noise(key_of[4], (D, W), D ** -0.5, 0.125, ((0, 64), (1, 8)), jnp.float32),
        "out_weight": noise(key_of[5], (W, D), W ** -0.5, 0.1875, ((0, 64), (1, 8)), jnp.float32),
        "value_basis": noise(key_of[6], (D, R), D ** -0.5, 0.125, ((0, 64),)),
        "out_basis": noise(key_of[7], (W, R), W ** -0.5, 0.1875, ((0, 64),)),
        "value_first": noise(key_of[8], (R, W), 1.0, 6.0, ((0, 64), (1, 8)), jnp.float32),
        "value_second": jnp.clip(jnp.exp(math.log(2.0) - 1.3862944 * jax.random.uniform(key_of[9], (R, W), jnp.float32) ** levels(key_of[9], (R, W), ((0, 64), (1, 8)), -0.2, 0.2)), 0.5, 2.0),
        "out_first": noise(key_of[10], (R, D), 1.0, 6.0, ((0, 64), (1, 8)), jnp.float32),
        "out_second": jnp.clip(jnp.exp(math.log(2.0) - 1.3862944 * jax.random.uniform(key_of[11], (R, D), jnp.float32) ** levels(key_of[11], (R, D), ((0, 64), (1, 8)), -0.2, 0.2)), 0.5, 2.0),
    }


first_decay = 0.8
second_decay = 0.9
step_rate = 0.1

def contract(left, right, precision=None):
    return lax.dot_general(left, right, (((0,), (0,)), ((), ())), preferred_element_type=jnp.float32, precision=precision)

def moments(projected, first, second):
    first_new = first_decay * first + (1.0 - first_decay) * projected
    second_new = second_decay * second + (1.0 - second_decay) * projected * projected
    return (first_new, second_new, first_new / jnp.sqrt(second_new))

def reference(layer_input, value_cotangent, mixed_output, output_cotangent, value_weight, out_weight, value_basis, out_basis, value_first, value_second, out_first, out_second):
    highest = lax.Precision.HIGHEST
    value_grad = contract(layer_input, value_cotangent)
    out_grad = contract(mixed_output, output_cotangent)
    value_proj = contract(value_basis.astype(jnp.float32), value_grad, highest)
    out_proj = contract(out_basis.astype(jnp.float32), out_grad, highest)
    value_first_new, value_second_new, value_dir = moments(value_proj, value_first, value_second)
    out_first_new, out_second_new, out_dir = moments(out_proj, out_first, out_second)
    total = jnp.sum(value_dir * value_dir) + jnp.sum(out_dir * out_dir)
    scale = step_rate / jnp.sqrt(1.0 + total / (R * (W + D)))
    value_step = scale * jnp.dot(value_basis.astype(jnp.float32), value_dir, precision=highest)
    out_step = scale * jnp.dot(out_basis.astype(jnp.float32), out_dir, precision=highest)
    value_new = value_weight - value_step
    out_new = out_weight - out_step
    return (value_new, out_new, value_step, out_step, value_new.astype(jnp.bfloat16), out_new.astype(jnp.bfloat16), value_first_new, value_second_new, out_first_new, out_second_new)
```

```python
import jax
import jax.numpy as jnp
from jax import lax
from jax.sharding import Mesh
from jax.sharding import PartitionSpec as P


D = 2048
W = 1024
R = 256
FS = ("fs_0", "fs_1")
TP = ("tp_0", "tp_1")
CORE = "tp_1"

first_decay = 0.8
second_decay = 0.9
step_rate = 0.1


def contract(left, right):
    return lax.dot_general(
        left, right, (((0,), (0,)), ((), ())), preferred_element_type=jnp.float32
    )


def sent_to_all(x, axis):
    peers = lax.axis_size(axis)
    return lax.all_to_all(jnp.broadcast_to(x[None], (peers, *x.shape)), axis, 0, 0, tiled=True)


def parts_of(wide, count):
    parts = []
    for _ in range(count):
        part = lax.reduce_precision(wide, 8, 7)
        parts.append(part.astype(jnp.bfloat16))
        wide = wide - part
    return parts


def moments(projected, first, second):
    first_new = first_decay * first + (1.0 - first_decay) * projected
    second_new = second_decay * second + (1.0 - second_decay) * projected * projected
    return (first_new, second_new, first_new / jnp.sqrt(second_new))


def local(
    layer_input,
    value_cotangent,
    mixed_output,
    output_cotangent,
    value_weight,
    out_weight,
    value_basis,
    out_basis,
    value_first,
    value_second,
    out_first,
    out_second,
):
    value_rows, value_cols = value_weight.shape
    out_rows, out_cols = out_weight.shape
    half = R // 2
    core = lax.axis_index(CORE)

    weight_tile = jnp.concatenate(
        [value_weight, out_weight[:, :value_cols], out_weight[:, value_cols:]], axis=0
    )
    weights = lax.all_gather(weight_tile[None], FS, axis=0, tiled=True)

    basis_tile = jnp.concatenate([value_basis, out_basis], axis=0)
    mine = sent_to_all(
        jnp.where(core == 0, basis_tile[:, :half], basis_tile[:, half:]), FS
    )
    other = lax.ppermute(mine, CORE, [(0, 1), (1, 0)])
    basis = jnp.where(
        core == 0,
        jnp.concatenate([mine, other], axis=2),
        jnp.concatenate([other, mine], axis=2),
    )
    basis_value = basis[:, :value_rows].reshape(-1, R)
    basis_out = basis[:, value_rows:].reshape(-1, R)

    value_grad = contract(layer_input, value_cotangent)
    out_grad = contract(mixed_output, output_cotangent)
    value_upper, value_lower = parts_of(value_grad, 2)
    out_upper, out_lower = parts_of(out_grad, 2)
    value_part = contract(basis_value, value_upper) + contract(basis_value, value_lower)
    out_part = contract(basis_out, out_upper) + contract(basis_out, out_lower)

    part = jnp.concatenate([value_part, out_part], axis=1)
    peers = lax.axis_size(FS)
    part = part.reshape(peers, R // peers, part.shape[1])
    projected = lax.all_to_all(part, FS, 0, 0, tiled=True).sum(axis=0)
    value_first_new, value_second_new, value_dir = moments(
        projected[:, :value_cols], value_first, value_second
    )
    out_first_new, out_second_new, out_dir = moments(
        projected[:, value_cols:], out_first, out_second
    )
    dirs = sent_to_all(jnp.concatenate([value_dir, out_dir], axis=1), FS).reshape(R, -1)
    squares = jnp.full((1, 128), jnp.sum(dirs * dirs))
    total = sent_to_all(squares, TP)[:, 0, 0].sum()
    scale = step_rate / jnp.sqrt(1.0 + total / (R * (W + D)))

    dir_parts = parts_of(dirs, 3)

    def stepped(rows, cols):
        return sum(
            jnp.dot(rows, part[:, cols], preferred_element_type=jnp.float32)
            for part in dir_parts
        )

    value_cut, out_cut = slice(0, value_cols), slice(value_cols, None)
    value_step = scale * stepped(value_basis, value_cut)
    out_step = scale * stepped(out_basis, out_cut)
    value_new = value_weight - value_step
    out_new = out_weight - out_step
    whole_value = weights[:, :value_rows].reshape(-1, value_cols)
    whole_out = jnp.concatenate(
        [
            weights[:, value_rows : value_rows + out_rows].reshape(-1, value_cols),
            weights[:, value_rows + out_rows :].reshape(-1, value_cols),
        ],
        axis=1,
    )
    value_copy = (whole_value - scale * stepped(basis_value, value_cut)).astype(jnp.bfloat16)
    out_copy = (whole_out - scale * stepped(basis_out, out_cut)).astype(jnp.bfloat16)
    return (
        value_new,
        out_new,
        value_step,
        out_step,
        value_copy,
        out_copy,
        value_first_new,
        value_second_new,
        out_first_new,
        out_second_new,
    )


def solution(mesh):
    torus = Mesh(mesh.devices.reshape(8, 8, 4, 2), ("fs_0", "fs_1", "tp_0", "tp_1"))
    rows = P(FS, None)
    tile = P(FS, TP)
    return jax.shard_map(
        local,
        mesh=torus,
        in_specs=(rows, tile, rows, tile, tile, tile, rows, rows, tile, tile, tile, tile),
        out_specs=(tile, tile, tile, tile, P(None, TP), P(None, TP), tile, tile, tile, tile),
        check_vma=False,
    )
```

```python
import jax
import jax.numpy as jnp
from jax import lax
from jax.experimental import pallas as pl
from jax.experimental.pallas import tpu as pltpu
from jax.sharding import Mesh
from jax.sharding import PartitionSpec as P


D = 2048
W = 1024
R = 256
FS = ("fs_0", "fs_1")
TP = ("tp_0", "tp_1")
CORE = "tp_1"
LANES = 128

first_decay = 0.8
second_decay = 0.9
step_rate = 0.1

F32 = jnp.float32
BF16 = jnp.bfloat16


def in_vmem(count):
    return [pl.BlockSpec(memory_space=pltpu.VMEM)] * count


def with_place(kernel, outs, vmem_inputs, name, flops=0):
    return pl.pallas_call(
        kernel,
        out_shape=[jax.ShapeDtypeStruct(shape, dtype) for shape, dtype in outs],
        in_specs=[pl.BlockSpec(memory_space=pltpu.SMEM), *in_vmem(vmem_inputs)],
        out_specs=in_vmem(len(outs)),
        name=name,
        cost_estimate=pl.CostEstimate(flops=flops, bytes_accessed=1 << 20, transcendentals=0),
    )


def parts_of(wide, count):
    parts = []
    for _ in range(count):
        part = wide.astype(BF16)
        parts.append(part)
        wide = wide - part.astype(F32)
    return parts


def tiles_to_send(place, value_weight, out_weight, value_basis, out_basis, weights, bases):
    core = place[0]
    weights[0:32, :] = value_weight[...]
    weights[32:48, :] = out_weight[:, :LANES]
    weights[48:64, :] = out_weight[:, LANES:]
    lower = jnp.concatenate([value_basis[:, :LANES], out_basis[:, :LANES]], axis=0)
    upper = jnp.concatenate([value_basis[:, LANES:], out_basis[:, LANES:]], axis=0)
    mine = jnp.where(core == 0, lower.astype(F32), upper.astype(F32)).astype(BF16)
    bases[...] = jnp.broadcast_to(mine[None], bases.shape)


def whole_rows(mine, other):
    value = jnp.concatenate(
        [mine[:, :32, :].reshape(-1, LANES), other[:, :32, :].reshape(-1, LANES)], axis=1
    )
    out = jnp.concatenate(
        [mine[:, 32:, :].reshape(-1, LANES), other[:, 32:, :].reshape(-1, LANES)], axis=1
    )
    return value, out


def projections(place, mine, other, value_grad, out_grad, parts):
    core = place[0]
    value_basis, out_basis = whole_rows(mine, other)

    def projected(grad, basis):
        rows = grad.shape[0]
        both = jnp.concatenate(parts_of(grad[...], 2), axis=0)
        sums = jnp.dot(both, basis, preferred_element_type=F32)
        return sums[:rows] + sums[rows:]

    flipped = jnp.concatenate(
        [projected(value_grad, value_basis), projected(out_grad, out_basis)], axis=0
    )
    peers = parts.shape[0] // 2
    for at, begin in ((core * peers, 0), ((1 - core) * peers, LANES)):
        rows = flipped[:, begin : begin + LANES].T
        parts[pl.ds(at, peers)] = rows.reshape(peers, rows.shape[0] // peers, rows.shape[1])


def directions(
    place,
    arrived,
    value_first,
    value_second,
    out_first,
    out_second,
    value_first_new,
    value_second_new,
    out_first_new,
    out_second_new,
    sent,
):
    total = jnp.sum(arrived[...], axis=0)

    def moments(projected, first, second, first_new, second_new):
        first_now = first_decay * first[...] + (1.0 - first_decay) * projected
        second_now = second_decay * second[...] + (1.0 - second_decay) * projected * projected
        first_new[...] = first_now
        second_new[...] = second_now
        return first_now / jnp.sqrt(second_now)

    value_dir = moments(
        total[:, :LANES], value_first, value_second, value_first_new, value_second_new
    )
    out_dir = moments(total[:, LANES:], out_first, out_second, out_first_new, out_second_new)
    both = jnp.concatenate([value_dir, out_dir], axis=1)
    sent[...] = jnp.broadcast_to(both[None], sent.shape)


def squares(place, dirs, sums):
    rows = jnp.sum(dirs[...] * dirs[...], axis=0)
    sums[...] = jnp.full(sums.shape, jnp.sum(rows), F32)


def raw_steps(place, mine, other, dirs, value_raw, out_raw):
    core = place[0]
    value_basis, out_basis = whole_rows(mine, other)
    peers = dirs.shape[0] // 2
    rows = jnp.concatenate(
        [
            dirs[pl.ds(core * peers, peers)].reshape(LANES, -1),
            dirs[pl.ds((1 - core) * peers, peers)].reshape(LANES, -1),
        ],
        axis=0,
    )

    def stepped(basis, cut):
        cols = cut.shape[1]
        sums = jnp.dot(
            basis, jnp.concatenate(parts_of(cut, 3), axis=1), preferred_element_type=F32
        )
        return sums[:, :cols] + sums[:, cols : 2 * cols] + sums[:, 2 * cols :]

    value_raw[...] = stepped(value_basis, rows[:, :LANES]).reshape(value_raw.shape)
    out_raw[...] = stepped(out_basis, rows[:, LANES:]).reshape(out_raw.shape)


def updates(
    place,
    sums,
    value_raw,
    out_raw,
    value_weight,
    out_weight,
    weights,
    value_new,
    out_new,
    value_step,
    out_step,
    value_copy,
    out_copy,
):
    shard = place[1]
    total = jnp.sum(sums[:, 0, :], axis=0, keepdims=True)
    scale = step_rate / jnp.sqrt(1.0 + total / (R * (W + D)))
    wide = jnp.concatenate([scale, scale], axis=1)
    value_now = scale * value_raw[shard]
    out_now = wide * out_raw[shard]
    value_step[...] = value_now
    out_step[...] = out_now
    value_new[...] = value_weight[...] - value_now
    out_new[...] = out_weight[...] - out_now
    value_copy[...] = (weights[:, :32, :] - scale[None] * value_raw[...]).astype(BF16)
    whole_out = jnp.concatenate([weights[:, 32:48, :], weights[:, 48:, :]], axis=2)
    out_copy[...] = (whole_out - wide[None] * out_raw[...]).astype(BF16)


def sent_across(x, axis):
    return lax.all_to_all(x, axis, 0, 0, tiled=True)


def local(
    layer_input,
    value_cotangent,
    mixed_output,
    output_cotangent,
    value_weight,
    out_weight,
    value_basis,
    out_basis,
    value_first,
    value_second,
    out_first,
    out_second,
):
    peers = lax.axis_size(FS)
    place = jnp.stack([lax.axis_index(CORE), lax.axis_index(FS)]).astype(jnp.int32)
    weight_tile, basis_tiles = with_place(
        tiles_to_send, [((64, LANES), F32), ((peers, 48, LANES), BF16)], 4, "tiles_to_send"
    )(place, value_weight, out_weight, value_basis, out_basis)
    weights = lax.all_gather(weight_tile[None], FS, axis=0, tiled=True)

    mine = sent_across(basis_tiles, FS)
    other = lax.ppermute(mine, CORE, [(0, 1), (1, 0)])

    def grad(cotangent, source):
        return lax.dot_general(
            cotangent, source, (((0,), (0,)), ((), ())), preferred_element_type=F32
        )

    value_grad = grad(value_cotangent, layer_input)
    out_grad = grad(output_cotangent, mixed_output)
    cols = 3 * LANES
    (parts,) = with_place(projections, [((peers, R // peers, cols), F32)], 4, "projections")(
        place, mine, other, value_grad, out_grad
    )
    arrived = sent_across(parts, FS)
    moment = [(value_first.shape, F32)] * 2 + [(out_first.shape, F32)] * 2
    *new_moments, sent = with_place(
        directions, [*moment, (parts.shape, F32)], 5, "directions"
    )(place, arrived, value_first, value_second, out_first, out_second)
    dirs = sent_across(sent, FS)
    (sums,) = with_place(squares, [((8, 1, LANES), F32)], 1, "squares")(place, dirs)
    all_sums = sent_across(sums, TP)
    value_raw, out_raw = with_place(
        raw_steps,
        [((peers, 32, LANES), F32), ((peers, 16, 2 * LANES), F32)],
        3,
        "raw_steps",
        flops=10**7,
    )(place, mine, other, dirs)
    value_new, out_new, value_step, out_step, value_copy, out_copy = with_place(
        updates,
        [
            (value_weight.shape, F32),
            (out_weight.shape, F32),
            (value_weight.shape, F32),
            (out_weight.shape, F32),
            ((peers, 32, LANES), BF16),
            ((peers, 16, 2 * LANES), BF16),
        ],
        6,
        "updates",
    )(place, all_sums, value_raw, out_raw, value_weight, out_weight, weights)
    return (
        value_new,
        out_new,
        value_step,
        out_step,
        value_copy.reshape(-1, LANES),
        out_copy.reshape(-1, 2 * LANES),
        *new_moments,
    )


def solution(mesh):
    torus = Mesh(mesh.devices.reshape(8, 8, 4, 2), ("fs_0", "fs_1", "tp_0", "tp_1"))
    rows = P(FS, None)
    tile = P(FS, TP)
    return jax.shard_map(
        local,
        mesh=torus,
        in_specs=(rows, tile, rows, tile, tile, tile, rows, rows, tile, tile, tile, tile),
        out_specs=(tile, tile, tile, tile, P(None, TP), P(None, TP), tile, tile, tile, tile),
        check_vma=False,
    )
```

```python
import jax
import jax.numpy as jnp
from jax import lax
from jax.experimental import pallas as pl
from jax.experimental.pallas import tpu as pltpu
from jax.sharding import Mesh
from jax.sharding import PartitionSpec as P


D = 2048
W = 1024
R = 256
FS = ("fs_0", "fs_1")
TP = ("tp_0", "tp_1")
CORE = "tp_1"
LANES = 128

first_decay = 0.8
second_decay = 0.9
step_rate = 0.1

F32 = jnp.float32
BF16 = jnp.bfloat16


def near(shape, dtype):
    return pltpu.VMEM(shape, dtype)


def far(shape, dtype):
    return jax.ShapeDtypeStruct(shape, dtype)


def run(kernel, outs, *args, flops=0, hbm=(), hbm_outs=(), **options):
    def spec(whether):
        return pl.BlockSpec(memory_space=pltpu.HBM if whether else pltpu.VMEM)

    return pl.pallas_call(
        kernel,
        out_shape=outs,
        in_specs=[spec(at in hbm) for at in range(len(args))],
        out_specs=[spec(at in hbm_outs) for at in range(len(outs))],
        name=kernel.__name__,
        compiler_params=pltpu.CompilerParams(vmem_limit_bytes=16 << 20),
        cost_estimate=pl.CostEstimate(flops=flops, bytes_accessed=1 << 20, transcendentals=0),
        **options,
    )(
        *(
            pltpu.with_memory_space_constraint(x, pltpu.HBM if at in hbm else pltpu.VMEM)
            for at, x in enumerate(args)
        )
    )


def parts_of(wide, count):
    parts = []
    for _ in range(count):
        part = wide.astype(BF16)
        parts.append(part)
        wide = wide - part.astype(F32)
    return parts


def tiles_to_send(value_weight, out_weight, value_basis, out_basis, weights, bases):
    core = lax.axis_index(CORE)
    weights[0:32, :] = value_weight[...]
    weights[32:48, :] = out_weight[:, :LANES]
    weights[48:64, :] = out_weight[:, LANES:]
    lower = jnp.concatenate([value_basis[:, :LANES], out_basis[:, :LANES]], axis=0)
    upper = jnp.concatenate([value_basis[:, LANES:], out_basis[:, LANES:]], axis=0)
    mine = jnp.where(core == 0, lower.astype(F32), upper.astype(F32)).astype(BF16)
    bases[...] = jnp.broadcast_to(mine[None], bases.shape)


def both_rows(basis):
    return basis[:, :32, :].reshape(-1, LANES), basis[:, 32:, :].reshape(-1, LANES)


def projected(half, basis, value_grad, out_grad, parts):
    def part(grad, rows):
        count = grad.shape[0]
        both = jnp.concatenate(parts_of(grad[...], 2), axis=0)
        sums = jnp.dot(both, rows, preferred_element_type=F32)
        return sums[:count] + sums[count:]

    value_basis, out_basis = both_rows(basis)
    flipped = jnp.concatenate([part(value_grad, value_basis), part(out_grad, out_basis)], axis=0)
    peers = parts.shape[0] // 2
    parts[pl.ds(half * peers, peers)] = flipped.T.reshape(peers, LANES // peers, -1)


def own_half(basis, value_grad, out_grad, parts):
    projected(lax.axis_index(CORE), basis, value_grad, out_grad, parts)


def other_half(basis, value_grad, out_grad, begun, parts):
    projected(1 - lax.axis_index(CORE), basis, value_grad, out_grad, parts)


def directions(
    arrived,
    value_first,
    value_second,
    out_first,
    out_second,
    value_first_new,
    value_second_new,
    out_first_new,
    out_second_new,
    sent,
):
    total = jnp.sum(arrived[...], axis=0)

    def moments(projected, first, second, first_new, second_new):
        first_now = first_decay * first[...] + (1.0 - first_decay) * projected
        second_now = second_decay * second[...] + (1.0 - second_decay) * projected * projected
        first_new[...] = first_now
        second_new[...] = second_now
        return first_now / jnp.sqrt(second_now)

    value_dir = moments(
        total[:, :LANES], value_first, value_second, value_first_new, value_second_new
    )
    out_dir = moments(total[:, LANES:], out_first, out_second, out_first_new, out_second_new)
    both = jnp.concatenate([value_dir, out_dir], axis=1)
    sent[...] = jnp.broadcast_to(both[None], sent.shape)


def squares(dirs, sums):
    rows = jnp.sum(dirs[...] * dirs[...], axis=0)
    sums[...] = jnp.full(sums.shape, jnp.sum(rows), F32)


def updates(
    mine,
    other,
    dirs,
    sums,
    value_weight,
    out_weight,
    far_weights,
    value_new,
    out_new,
    value_step,
    out_step,
    far_value_copy,
    far_out_copy,
    weights,
    value_whole,
    out_whole,
    value_copy,
    out_copy,
    sems,
):
    fetch = pltpu.make_async_copy(far_weights, weights, sems.at[0])
    fetch.start()
    core = lax.axis_index(CORE)
    shard = lax.axis_index(FS)
    value_basis, out_basis = (
        jnp.concatenate(halves, axis=1) for halves in zip(both_rows(mine), both_rows(other))
    )
    peers = dirs.shape[0] // 2
    rows = jnp.concatenate(
        [
            dirs[pl.ds(core * peers, peers)].reshape(LANES, -1),
            dirs[pl.ds((1 - core) * peers, peers)].reshape(LANES, -1),
        ],
        axis=0,
    )
    total = jnp.sum(sums[:, 0, :], axis=0, keepdims=True)
    scale = step_rate / jnp.sqrt(1.0 + total / (R * (W + D)))

    def stepped(basis, cut, scale):
        cols = cut.shape[1]
        sums = jnp.dot(
            basis, jnp.concatenate(parts_of(cut, 3), axis=1), preferred_element_type=F32
        )
        return scale * (sums[:, :cols] + sums[:, cols : 2 * cols] + sums[:, 2 * cols :])

    value_whole[...] = stepped(value_basis, rows[:, :LANES], scale).reshape(value_whole.shape)
    fetch.wait()
    value_copy[...] = (weights[:, :32, :] - value_whole[...]).astype(BF16)
    value_out = pltpu.make_async_copy(value_copy, far_value_copy, sems.at[1])
    value_out.start()
    value_step[...] = value_whole[shard]
    value_new[...] = value_weight[...] - value_whole[shard]
    wide = jnp.concatenate([scale, scale], axis=1)
    out_whole[...] = stepped(out_basis, rows[:, LANES:], wide).reshape(out_whole.shape)
    out_copy[:, :, :LANES] = (weights[:, 32:48, :] - out_whole[:, :, :LANES]).astype(BF16)
    out_copy[:, :, LANES:] = (weights[:, 48:, :] - out_whole[:, :, LANES:]).astype(BF16)
    out_out = pltpu.make_async_copy(out_copy, far_out_copy, sems.at[2])
    out_out.start()
    out_step[...] = out_whole[shard]
    out_new[...] = out_weight[...] - out_whole[shard]
    value_out.wait()
    out_out.wait()


def sent_across(x, axis):
    return lax.all_to_all(x, axis, 0, 0, tiled=True)


def local(
    layer_input,
    value_cotangent,
    mixed_output,
    output_cotangent,
    value_weight,
    out_weight,
    value_basis,
    out_basis,
    value_first,
    value_second,
    out_first,
    out_second,
):
    peers = lax.axis_size(FS)
    weight_tile, basis_tiles = run(
        tiles_to_send,
        [far((64, LANES), F32), far((peers, 48, LANES), BF16)],
        value_weight,
        out_weight,
        value_basis,
        out_basis,
    )
    weights = lax.all_gather(weight_tile[None], FS, axis=0, tiled=True)

    mine = sent_across(basis_tiles, FS)
    other = lax.ppermute(mine, CORE, [(0, 1), (1, 0)])

    def grad(cotangent, source):
        return lax.dot_general(
            cotangent, source, (((0,), (0,)), ((), ())), preferred_element_type=F32
        )

    value_grad = grad(value_cotangent, layer_input)
    out_grad = grad(output_cotangent, mixed_output)
    parts = near((peers, R // peers, 3 * LANES), F32)
    (begun,) = run(own_half, [parts], mine, value_grad, out_grad, flops=10**10)
    (whole,) = run(
        other_half, [parts], other, value_grad, out_grad, begun, input_output_aliases={3: 0}
    )
    arrived = sent_across(whole, FS)
    moment = [far(value_first.shape, F32)] * 2 + [far(out_first.shape, F32)] * 2
    *new_moments, sent = run(
        directions,
        [*moment, parts],
        arrived,
        value_first,
        value_second,
        out_first,
        out_second,
    )
    dirs = sent_across(sent, FS)
    (sums,) = run(squares, [near((8, 1, LANES), F32)], dirs)
    all_sums = sent_across(sums, TP)
    value_whole, out_whole = (peers, 32, LANES), (peers, 16, 2 * LANES)
    *rows, value_copy, out_copy = run(
        updates,
        [
            far(value_weight.shape, F32),
            far(out_weight.shape, F32),
            far(value_weight.shape, F32),
            far(out_weight.shape, F32),
            far(value_whole, BF16),
            far(out_whole, BF16),
        ],
        mine,
        other,
        dirs,
        all_sums,
        value_weight,
        out_weight,
        weights,
        hbm=(6,),
        hbm_outs=(4, 5),
        scratch_shapes=[
            pltpu.VMEM(weights.shape, F32),
            pltpu.VMEM(value_whole, F32),
            pltpu.VMEM(out_whole, F32),
            pltpu.VMEM(value_whole, BF16),
            pltpu.VMEM(out_whole, BF16),
            pltpu.SemaphoreType.DMA((3,)),
        ],
    )
    return (
        *rows,
        value_copy.reshape(-1, LANES),
        out_copy.reshape(-1, 2 * LANES),
        *new_moments,
    )


def solution(mesh):
    torus = Mesh(mesh.devices.reshape(8, 8, 4, 2), ("fs_0", "fs_1", "tp_0", "tp_1"))
    rows = P(FS, None)
    tile = P(FS, TP)
    return jax.shard_map(
        local,
        mesh=torus,
        in_specs=(rows, tile, rows, tile, tile, tile, rows, rows, tile, tile, tile, tile),
        out_specs=(tile, tile, tile, tile, P(None, TP), P(None, TP), tile, tile, tile, tile),
        check_vma=False,
    )
```

```python
import jax
import jax.numpy as jnp
from jax import lax
from jax.experimental import pallas as pl
from jax.experimental.pallas import tpu as pltpu
from jax.sharding import Mesh
from jax.sharding import PartitionSpec as P

D = 2048
W = 1024
R = 256
FS = ("fs_0", "fs_1")
TP = ("tp_0", "tp_1")
ALL = FS + TP
CORE = "tp_1"
LANES = 128

first_decay = 0.8
second_decay = 0.9
step_rate = 0.1

F32 = jnp.float32
BF16 = jnp.bfloat16


SIDE = 8
BASIS_ROWS = 48
WEIGHT_ROWS = 64


def device_of(z, y, x, core):
    return ((z % SIDE * SIDE + y % SIDE) * 4 + x) * 2 + core


def far_groups():
    return [
        [device_of(z, y, x, core) for z in range(odd_z, SIDE, 2) for y in range(odd_y, SIDE, 2)]
        for x in range(4)
        for core in range(2)
        for odd_z in range(2)
        for odd_y in range(2)
    ]


def near_groups():
    def block(z, y, x, core):
        rows = (z + 2 * core, z + 1)
        cols = (y + 2 * core, y + 1)
        return [device_of(row, col, x, core) for row in rows for col in cols]

    return [
        block(z, y, x, core)
        for x in range(4)
        for core in range(2)
        for z in range(0, SIDE, 2)
        for y in range(0, SIDE, 2)
    ]


def place_of(shard):
    z, y = divmod(shard, SIDE)
    return ((z % 2 * 2 + y % 2) * 4 + z // 2) * 4 + y // 2


def near(shape, dtype):
    return pltpu.VMEM(shape, dtype)


def far(shape, dtype):
    return jax.ShapeDtypeStruct(shape, dtype)


def run(kernel, outs, *args, flops=0, hbm=(), hbm_outs=(), **options):
    def spec(whether):
        return pl.BlockSpec(memory_space=pltpu.HBM if whether else pltpu.VMEM)

    return pl.pallas_call(
        kernel,
        out_shape=outs,
        in_specs=[spec(at in hbm) for at in range(len(args))],
        out_specs=[spec(at in hbm_outs) for at in range(len(outs))],
        name=kernel.__name__,
        compiler_params=pltpu.CompilerParams(vmem_limit_bytes=16 << 20),
        cost_estimate=pl.CostEstimate(flops=flops, bytes_accessed=1 << 20, transcendentals=0),
        **options,
    )(
        *(
            pltpu.with_memory_space_constraint(x, pltpu.HBM if at in hbm else pltpu.VMEM)
            for at, x in enumerate(args)
        )
    )


def parts_of(wide, count):
    parts = []
    for _ in range(count):
        part = wide.astype(BF16)
        parts.append(part)
        wide = wide - part.astype(F32)
    return parts


def tiles_to_send(
    far_value_weight,
    far_out_weight,
    far_value_basis,
    far_out_basis,
    tiles,
    value_weight,
    out_weight,
    value_basis,
    out_basis,
    sems,
):
    pairs = (
        (far_value_basis, value_basis),
        (far_out_basis, out_basis),
        (far_value_weight, value_weight),
        (far_out_weight, out_weight),
    )
    copies = [pltpu.make_async_copy(a, b, sems.at[at]) for at, (a, b) in enumerate(pairs)]
    for copy in copies:
        copy.start()
    for copy in copies:
        copy.wait()
    lower = jnp.concatenate([value_basis[:, :LANES], out_basis[:, :LANES]], axis=0)
    upper = jnp.concatenate([value_basis[:, LANES:], out_basis[:, LANES:]], axis=0)
    mine = jnp.where(lax.axis_index(CORE) == 0, lower.astype(F32), upper.astype(F32))
    weights = jnp.concatenate(
        [value_weight[...], out_weight[:, :LANES], out_weight[:, LANES:]], axis=0
    )
    tile = jnp.concatenate([mine.astype(BF16), *parts_of(weights, 2)], axis=0)
    tiles[...] = jnp.broadcast_to(tile[None], tiles.shape)


def both_rows(basis):
    places = [place_of(shard) for shard in range(basis.shape[0])]
    return (
        jnp.concatenate([basis[at, :32, :] for at in places], axis=0),
        jnp.concatenate([basis[at, 32:, :] for at in places], axis=0),
    )


def projected(half, basis, value_grad, out_grad, parts):
    def part(grad, rows):
        count = grad.shape[0]
        both = jnp.concatenate(parts_of(grad[...], 2), axis=0)
        sums = jnp.dot(both, rows, preferred_element_type=F32)
        return sums[:count] + sums[count:]

    value_basis, out_basis = both_rows(basis)
    flipped = jnp.concatenate([part(value_grad, value_basis), part(out_grad, out_basis)], axis=0)
    peers = parts.shape[0] // 2
    parts[pl.ds(half * peers, peers)] = flipped.T.reshape(peers, LANES // peers, -1)


def own_half(basis, value_grad, out_grad, parts):
    projected(lax.axis_index(CORE), basis, value_grad, out_grad, parts)


def other_half(basis, value_grad, out_grad, begun, parts):
    projected(1 - lax.axis_index(CORE), basis, value_grad, out_grad, parts)


def directions(
    arrived,
    value_first,
    value_second,
    out_first,
    out_second,
    value_first_new,
    value_second_new,
    out_first_new,
    out_second_new,
    sent,
):
    total = jnp.sum(arrived[...], axis=0)

    def moments(projected, first, second, first_new, second_new):
        first_now = first_decay * first[...] + (1.0 - first_decay) * projected
        second_now = second_decay * second[...] + (1.0 - second_decay) * projected * projected
        first_new[...] = first_now
        second_new[...] = second_now
        return first_now / jnp.sqrt(second_now)

    value_dir = moments(
        total[:, :LANES], value_first, value_second, value_first_new, value_second_new
    )
    out_dir = moments(total[:, LANES:], out_first, out_second, out_first_new, out_second_new)
    both = jnp.concatenate([value_dir, out_dir], axis=1)
    sent[...] = jnp.broadcast_to(both[None], sent.shape)


def squares(dirs, sums):
    rows = jnp.sum(dirs[...] * dirs[...], axis=0)
    sums[...] = jnp.full(sums.shape, jnp.sum(rows), F32)


def updates(
    mine,
    other,
    dirs,
    sums,
    value_weight,
    out_weight,
    far_tiles,
    value_new,
    out_new,
    value_step,
    out_step,
    far_value_copy,
    far_out_copy,
    weights,
    value_whole,
    out_whole,
    value_copy,
    out_copy,
    sems,
):
    fetch = pltpu.make_async_copy(far_tiles.at[:, BASIS_ROWS:, :], weights, sems.at[0])
    fetch.start()
    core = lax.axis_index(CORE)
    shard = lax.axis_index(FS)
    value_basis, out_basis = (
        jnp.concatenate(halves, axis=1) for halves in zip(both_rows(mine), both_rows(other))
    )
    peers = dirs.shape[0] // 2
    rows = jnp.concatenate(
        [
            dirs[pl.ds(core * peers, peers)].reshape(LANES, -1),
            dirs[pl.ds((1 - core) * peers, peers)].reshape(LANES, -1),
        ],
        axis=0,
    )
    total = jnp.sum(sums[:, 0, :], axis=0, keepdims=True)
    scale = step_rate / jnp.sqrt(1.0 + total / (R * (W + D)))

    def stepped(basis, cut, scale):
        cols = cut.shape[1]
        sums = jnp.dot(
            basis, jnp.concatenate(parts_of(cut, 3), axis=1), preferred_element_type=F32
        )
        return scale * (sums[:, :cols] + sums[:, cols : 2 * cols] + sums[:, 2 * cols :])

    value_whole[...] = stepped(value_basis, rows[:, :LANES], scale).reshape(value_whole.shape)
    fetch.wait()


    def whole(at, rows):
        lower = slice(WEIGHT_ROWS + rows.start, WEIGHT_ROWS + rows.stop)
        return weights[at, rows, :].astype(F32) + weights[at, lower, :].astype(F32)

    places = [place_of(peer) for peer in range(2 * peers)]
    for peer, at in enumerate(places):
        value_copy[peer] = (whole(at, slice(0, 32)) - value_whole[peer]).astype(BF16)
    value_out = pltpu.make_async_copy(value_copy, far_value_copy, sems.at[1])
    value_out.start()
    value_step[...] = value_whole[shard]
    value_new[...] = value_weight[...] - value_whole[shard]
    wide = jnp.concatenate([scale, scale], axis=1)
    out_whole[...] = stepped(out_basis, rows[:, LANES:], wide).reshape(out_whole.shape)
    for peer, at in enumerate(places):
        for rows, lanes in ((slice(32, 48), slice(0, LANES)), (slice(48, 64), slice(LANES, None))):
            step = out_whole[peer, :, lanes]
            out_copy[peer, :, lanes] = (whole(at, rows) - step).astype(BF16)
    out_out = pltpu.make_async_copy(out_copy, far_out_copy, sems.at[2])
    out_out.start()
    out_step[...] = out_whole[shard]
    out_new[...] = out_weight[...] - out_whole[shard]
    value_out.wait()
    out_out.wait()


def sent_across(x, axis, groups=None):
    return lax.all_to_all(x, axis, 0, 0, tiled=True, axis_index_groups=groups)


def local(
    layer_input,
    value_cotangent,
    mixed_output,
    output_cotangent,
    value_weight,
    out_weight,
    value_basis,
    out_basis,
    value_first,
    value_second,
    out_first,
    out_second,
):
    peers = lax.axis_size(FS)
    tile_rows = BASIS_ROWS + 2 * WEIGHT_ROWS
    (tiles,) = run(
        tiles_to_send,
        [near((16, tile_rows, LANES), BF16)],
        value_weight,
        out_weight,
        value_basis,
        out_basis,
        hbm=(0, 1, 2, 3),
        scratch_shapes=[
            pltpu.VMEM(value_weight.shape, F32),
            pltpu.VMEM(out_weight.shape, F32),
            pltpu.VMEM(value_basis.shape, BF16),
            pltpu.VMEM(out_basis.shape, BF16),
            pltpu.SemaphoreType.DMA((4,)),
        ],
    )
    tiles = sent_across(tiles, ALL, far_groups())
    tiles = jnp.broadcast_to(tiles.reshape(1, -1, LANES), (4, 16 * tile_rows, LANES))
    tiles = sent_across(tiles, ALL, near_groups()).reshape(peers, tile_rows, LANES)

    mine = tiles[:, :BASIS_ROWS, :]
    other = lax.ppermute(mine, CORE, [(0, 1), (1, 0)])

    def grad(cotangent, source):
        return lax.dot_general(
            cotangent, source, (((0,), (0,)), ((), ())), preferred_element_type=F32
        )

    value_grad = grad(value_cotangent, layer_input)
    out_grad = grad(output_cotangent, mixed_output)
    parts = near((peers, R // peers, 3 * LANES), F32)
    (begun,) = run(own_half, [parts], mine, value_grad, out_grad, flops=10**10)
    (whole,) = run(
        other_half, [parts], other, value_grad, out_grad, begun, input_output_aliases={3: 0}
    )
    arrived = sent_across(whole, FS)
    moment = [far(value_first.shape, F32)] * 2 + [far(out_first.shape, F32)] * 2
    *new_moments, sent = run(
        directions,
        [*moment, parts],
        arrived,
        value_first,
        value_second,
        out_first,
        out_second,
    )
    dirs = sent_across(sent, FS)
    (sums,) = run(squares, [near((8, 1, LANES), F32)], dirs)
    all_sums = sent_across(sums, TP)
    value_whole, out_whole = (peers, 32, LANES), (peers, 16, 2 * LANES)
    *rows, value_copy, out_copy = run(
        updates,
        [
            far(value_weight.shape, F32),
            far(out_weight.shape, F32),
            far(value_weight.shape, F32),
            far(out_weight.shape, F32),
            far(value_whole, BF16),
            far(out_whole, BF16),
        ],
        mine,
        other,
        dirs,
        all_sums,
        value_weight,
        out_weight,
        tiles,
        hbm=(6,),
        hbm_outs=(4, 5),
        scratch_shapes=[
            pltpu.VMEM((peers, 2 * WEIGHT_ROWS, LANES), BF16),
            pltpu.VMEM(value_whole, F32),
            pltpu.VMEM(out_whole, F32),
            pltpu.VMEM(value_whole, BF16),
            pltpu.VMEM(out_whole, BF16),
            pltpu.SemaphoreType.DMA((3,)),
        ],
    )
    return (
        *rows,
        value_copy.reshape(-1, LANES),
        out_copy.reshape(-1, 2 * LANES),
        *new_moments,
    )


def solution(mesh):
    torus = Mesh(mesh.devices.reshape(8, 8, 4, 2), ("fs_0", "fs_1", "tp_0", "tp_1"))
    rows = P(FS, None)
    tile = P(FS, TP)
    return jax.shard_map(
        local,
        mesh=torus,
        in_specs=(rows, tile, rows, tile, tile, tile, rows, rows, tile, tile, tile, tile),
        out_specs=(tile, tile, tile, tile, P(None, TP), P(None, TP), tile, tile, tile, tile),
        check_vma=False,
    )
```

```python
import jax
import jax.numpy as jnp
from jax import lax
from jax.experimental import pallas as pl
from jax.experimental.pallas import tpu as pltpu
from jax.sharding import Mesh
from jax.sharding import PartitionSpec as P


D = 2048
W = 1024
R = 256
FS = ("fs_0", "fs_1")
TP = ("tp_0", "tp_1")
CORE = "tp_1"
LANES = 128

first_decay = 0.8
second_decay = 0.9
step_rate = 0.1

F32 = jnp.float32
BF16 = jnp.bfloat16


def near(shape, dtype):
    return pltpu.VMEM(shape, dtype)


def far(shape, dtype):
    return jax.ShapeDtypeStruct(shape, dtype)


def run(kernel, outs, *args, flops=0, hbm=(), hbm_outs=(), **options):
    def spec(whether):
        return pl.BlockSpec(memory_space=pltpu.HBM if whether else pltpu.VMEM)

    return pl.pallas_call(
        kernel,
        out_shape=outs,
        in_specs=[spec(at in hbm) for at in range(len(args))],
        out_specs=[spec(at in hbm_outs) for at in range(len(outs))],
        name=kernel.__name__,
        compiler_params=pltpu.CompilerParams(vmem_limit_bytes=16 << 20),
        cost_estimate=pl.CostEstimate(flops=flops, bytes_accessed=1 << 20, transcendentals=0),
        **options,
    )(
        *(
            pltpu.with_memory_space_constraint(x, pltpu.HBM if at in hbm else pltpu.VMEM)
            for at, x in enumerate(args)
        )
    )


def parts_of(wide, count):
    parts = []
    for _ in range(count):
        part = wide.astype(BF16)
        parts.append(part)
        wide = wide - part.astype(F32)
    return parts


def fetched(pairs, sems, first=0):
    copies = [pltpu.make_async_copy(a, b, sems.at[first + at]) for at, (a, b) in enumerate(pairs)]
    for copy in copies:
        copy.start()
    return copies


def tiles_to_send(
    far_value_weight,
    far_out_weight,
    far_value_basis,
    far_out_basis,
    weights,
    bases,
    out_weight,
    value_basis,
    out_basis,
    sems,
):
    rows = far_value_weight.shape[0]
    copies = fetched(
        (
            (far_value_basis, value_basis),
            (far_out_basis, out_basis),
            (far_out_weight, out_weight),
            (far_value_weight, weights.at[pl.ds(0, rows)]),
        ),
        sems,
    )
    for copy in copies:
        copy.wait()
    weights[32:48, :] = out_weight[:, :LANES]
    weights[48:64, :] = out_weight[:, LANES:]
    lower = jnp.concatenate([value_basis[:, :LANES], out_basis[:, :LANES]], axis=0)
    upper = jnp.concatenate([value_basis[:, LANES:], out_basis[:, LANES:]], axis=0)
    core = lax.axis_index(CORE)
    mine = jnp.where(core == 0, lower.astype(F32), upper.astype(F32)).astype(BF16)
    bases[...] = jnp.broadcast_to(mine[None], bases.shape)


def both_rows(basis):
    return basis[:, :32, :].reshape(-1, LANES), basis[:, 32:, :].reshape(-1, LANES)


def projected(half, out_rows, out_grad, value_rows, value_grad, parts):
    def part(grad, rows):
        count = grad.shape[0]
        both = jnp.concatenate(parts_of(grad[...], 2), axis=0)
        sums = jnp.dot(both, rows, preferred_element_type=F32)
        return sums[:count] + sums[count:]

    peers = parts.shape[0] // 2
    rows = pl.ds(half * peers, peers)
    shape = (peers, LANES // peers, -1)
    parts[rows, :, LANES:] = part(out_grad, out_rows).T.reshape(shape)
    parts[rows, :, :LANES] = part(value_grad(), value_rows).T.reshape(shape)


def own_half(far_basis, far_value_grad, out_grad, parts, value_grad, basis, sems):
    begun, grad_begun = fetched(((far_basis, basis), (far_value_grad, value_grad)), sems)

    def value_grad_now():
        grad_begun.wait()
        return value_grad

    begun.wait()
    value_rows, out_rows = both_rows(basis)
    projected(lax.axis_index(CORE), out_rows, out_grad, value_rows, value_grad_now, parts)


def other_half(basis, value_grad, out_grad, begun, parts):
    value_rows, out_rows = both_rows(basis)
    half = 1 - lax.axis_index(CORE)
    projected(half, out_rows, out_grad, value_rows, lambda: value_grad, parts)


def directions(
    arrived,
    value_first,
    value_second,
    out_first,
    out_second,
    value_first_new,
    value_second_new,
    out_first_new,
    out_second_new,
    sent,
):
    total = jnp.sum(arrived[...], axis=0)

    def moments(projected, first, second, first_new, second_new):
        first_now = first_decay * first[...] + (1.0 - first_decay) * projected
        second_now = second_decay * second[...] + (1.0 - second_decay) * projected * projected
        first_new[...] = first_now
        second_new[...] = second_now
        return first_now / jnp.sqrt(second_now)

    value_dir = moments(
        total[:, :LANES], value_first, value_second, value_first_new, value_second_new
    )
    out_dir = moments(total[:, LANES:], out_first, out_second, out_first_new, out_second_new)
    both = jnp.concatenate([value_dir, out_dir], axis=1)
    sent[...] = jnp.broadcast_to(both[None], sent.shape)


def squares(dirs, sums):
    rows = jnp.sum(dirs[...] * dirs[...], axis=0)
    sums[...] = jnp.full(sums.shape, jnp.sum(rows), F32)


def raw_steps(
    far_mine,
    far_other,
    dirs,
    far_value_raw,
    far_out_raw,
    bases,
    value_raw,
    out_raw,
    sems,
):
    copies = fetched(((far_mine, bases.at[0]), (far_other, bases.at[1])), sems)
    core = lax.axis_index(CORE)
    peers = dirs.shape[0] // 2
    rows = jnp.concatenate(
        [
            dirs[pl.ds(core * peers, peers)].reshape(LANES, -1),
            dirs[pl.ds((1 - core) * peers, peers)].reshape(LANES, -1),
        ],
        axis=0,
    )

    def stepped(basis, cut):
        cols = cut.shape[1]
        sums = jnp.dot(
            basis, jnp.concatenate(parts_of(cut, 3), axis=1), preferred_element_type=F32
        )
        return sums[:, :cols] + sums[:, cols : 2 * cols] + sums[:, 2 * cols :]

    for copy in copies:
        copy.wait()
    value_basis, out_basis = (
        jnp.concatenate(halves, axis=1) for halves in zip(*(both_rows(bases[at]) for at in (0, 1)))
    )
    value_raw[...] = stepped(value_basis, rows[:, :LANES]).reshape(value_raw.shape)
    sent = fetched(((value_raw, far_value_raw),), sems, 2)
    out_raw[...] = stepped(out_basis, rows[:, LANES:]).reshape(out_raw.shape)
    for copy in sent + fetched(((out_raw, far_out_raw),), sems, 3):
        copy.wait()


CHUNKS = 4


def updates(
    sums,
    value_weight,
    out_weight,
    far_value_raw,
    far_out_raw,
    far_weights,
    value_new,
    out_new,
    value_step,
    out_step,
    far_value_copy,
    far_out_copy,
    weights,
    value_raw,
    out_raw,
    value_copy,
    out_copy,
    sems,
):
    peers = far_weights.shape[0] // CHUNKS
    chunks = [pl.ds(at * peers, peers) for at in range(CHUNKS)]
    arriving = [
        fetched(
            [
                (far.at[chunk], local.at[chunk])
                for far, local in (
                    (far_weights, weights),
                    (far_value_raw, value_raw),
                    (far_out_raw, out_raw),
                )
            ],
            sems,
            3 * at,
        )
        for at, chunk in enumerate(chunks)
    ]
    total = jnp.sum(sums[:, 0, :], axis=0, keepdims=True)
    scale = step_rate / jnp.sqrt(1.0 + total / (R * (W + D)))
    wide = jnp.concatenate([scale, scale], axis=1)
    leaving = []
    for at, chunk in enumerate(chunks):
        for copy in arriving[at]:
            copy.wait()
        step = scale[None] * value_raw[chunk]
        value_copy[chunk] = (weights[chunk, :32, :] - step).astype(BF16)
        step = wide[None] * out_raw[chunk]
        out_copy[chunk, :, :LANES] = (weights[chunk, 32:48, :] - step[:, :, :LANES]).astype(BF16)
        out_copy[chunk, :, LANES:] = (weights[chunk, 48:, :] - step[:, :, LANES:]).astype(BF16)
        leaving += fetched(
            (
                (value_copy.at[chunk], far_value_copy.at[chunk]),
                (out_copy.at[chunk], far_out_copy.at[chunk]),
            ),
            sems,
            3 * CHUNKS + 2 * at,
        )
    shard = lax.axis_index(FS)
    value_now = scale * value_raw[shard]
    out_now = wide * out_raw[shard]
    value_step[...] = value_now
    out_step[...] = out_now
    value_new[...] = value_weight[...] - value_now
    out_new[...] = out_weight[...] - out_now
    for copy in leaving:
        copy.wait()


def sent_across(x, axis):
    return lax.all_to_all(x, axis, 0, 0, tiled=True)


def local(
    layer_input,
    value_cotangent,
    mixed_output,
    output_cotangent,
    value_weight,
    out_weight,
    value_basis,
    out_basis,
    value_first,
    value_second,
    out_first,
    out_second,
):
    peers = lax.axis_size(FS)
    semaphores = pltpu.SemaphoreType.DMA
    weight_tile, basis_tiles = run(
        tiles_to_send,
        [near((64, LANES), F32), far((peers, 48, LANES), BF16)],
        value_weight,
        out_weight,
        value_basis,
        out_basis,
        hbm=(0, 1, 2, 3),
        scratch_shapes=[
            pltpu.VMEM(out_weight.shape, F32),
            pltpu.VMEM(value_basis.shape, BF16),
            pltpu.VMEM(out_basis.shape, BF16),
            semaphores((4,)),
        ],
    )
    weights = lax.all_gather(weight_tile[None], FS, axis=0, tiled=True)

    mine = sent_across(basis_tiles, FS)
    other = lax.ppermute(mine, CORE, [(0, 1), (1, 0)])

    def grad(cotangent, source):
        return lax.dot_general(
            cotangent, source, (((0,), (0,)), ((), ())), preferred_element_type=F32
        )

    value_grad = grad(value_cotangent, layer_input)
    out_grad = grad(output_cotangent, mixed_output)
    parts = near((peers, R // peers, 3 * LANES), F32)
    begun, value_grad = run(
        own_half,
        [parts, near(value_grad.shape, F32)],
        mine,
        value_grad,
        out_grad,
        flops=10**10,
        hbm=(0, 1),
        scratch_shapes=[pltpu.VMEM(mine.shape, BF16), semaphores((2,))],
    )
    (whole,) = run(
        other_half, [parts], other, value_grad, out_grad, begun, input_output_aliases={3: 0}
    )
    arrived = sent_across(whole, FS)
    moment = [far(value_first.shape, F32)] * 2 + [far(out_first.shape, F32)] * 2
    *new_moments, sent = run(
        directions,
        [*moment, parts],
        arrived,
        value_first,
        value_second,
        out_first,
        out_second,
    )
    dirs = sent_across(sent, FS)
    (sums,) = run(squares, [near((8, 1, LANES), F32)], dirs)
    all_sums = sent_across(sums, TP)
    value_whole, out_whole = (peers, 32, LANES), (peers, 16, 2 * LANES)
    value_raw, out_raw = run(
        raw_steps,
        [pltpu.HBM(value_whole, F32), pltpu.HBM(out_whole, F32)],
        mine,
        other,
        dirs,
        flops=10**9,
        hbm=(0, 1),
        hbm_outs=(0, 1),
        scratch_shapes=[
            pltpu.VMEM((2, *mine.shape), BF16),
            pltpu.VMEM(value_whole, F32),
            pltpu.VMEM(out_whole, F32),
            semaphores((4,)),
        ],
    )
    *rows, value_copy, out_copy = run(
        updates,
        [
            far(value_weight.shape, F32),
            far(out_weight.shape, F32),
            far(value_weight.shape, F32),
            far(out_weight.shape, F32),
            far(value_whole, BF16),
            far(out_whole, BF16),
        ],
        all_sums,
        value_weight,
        out_weight,
        value_raw,
        out_raw,
        weights,
        hbm=(3, 4, 5),
        hbm_outs=(4, 5),
        scratch_shapes=[
            pltpu.VMEM(weights.shape, F32),
            pltpu.VMEM(value_whole, F32),
            pltpu.VMEM(out_whole, F32),
            pltpu.VMEM(value_whole, BF16),
            pltpu.VMEM(out_whole, BF16),
            semaphores((5 * CHUNKS,)),
        ],
    )
    return (
        *rows,
        value_copy.reshape(-1, LANES),
        out_copy.reshape(-1, 2 * LANES),
        *new_moments,
    )


def solution(mesh):
    torus = Mesh(mesh.devices.reshape(8, 8, 4, 2), ("fs_0", "fs_1", "tp_0", "tp_1"))
    rows = P(FS, None)
    tile = P(FS, TP)
    return jax.shard_map(
        local,
        mesh=torus,
        in_specs=(rows, tile, rows, tile, tile, tile, rows, rows, tile, tile, tile, tile),
        out_specs=(tile, tile, tile, tile, P(None, TP), P(None, TP), tile, tile, tile, tile),
        check_vma=False,
    )
```

```python
import jax
import jax.numpy as jnp
from jax import lax
from jax.experimental import pallas as pl
from jax.experimental.pallas import tpu as pltpu
from jax.sharding import Mesh
from jax.sharding import PartitionSpec as P


D = 2048
W = 1024
R = 256
FS = ("fs_0", "fs_1")
TP = ("tp_0", "tp_1")
CORE = "tp_1"
ALL = FS + TP
QUARTER = 24
LANES = 128

first_decay = 0.8
second_decay = 0.9
step_rate = 0.1

F32 = jnp.float32
BF16 = jnp.bfloat16


def near(shape, dtype):
    return pltpu.VMEM(shape, dtype)


def far(shape, dtype):
    return jax.ShapeDtypeStruct(shape, dtype)


def run(kernel, outs, *args, flops=0, hbm=(), hbm_outs=(), **options):
    def spec(whether):
        return pl.BlockSpec(memory_space=pltpu.HBM if whether else pltpu.VMEM)

    return pl.pallas_call(
        kernel,
        out_shape=outs,
        in_specs=[spec(at in hbm) for at in range(len(args))],
        out_specs=[spec(at in hbm_outs) for at in range(len(outs))],
        name=kernel.__name__,
        compiler_params=pltpu.CompilerParams(vmem_limit_bytes=16 << 20),
        cost_estimate=pl.CostEstimate(flops=flops, bytes_accessed=1 << 20, transcendentals=0),
        **options,
    )(
        *(
            pltpu.with_memory_space_constraint(x, pltpu.HBM if at in hbm else pltpu.VMEM)
            for at, x in enumerate(args)
        )
    )


def parts_of(wide, count):
    parts = []
    for _ in range(count):
        part = wide.astype(BF16)
        parts.append(part)
        wide = wide - part.astype(F32)
    return parts


def fetched(pairs, sems, first=0):
    copies = [pltpu.make_async_copy(a, b, sems.at[first + at]) for at, (a, b) in enumerate(pairs)]
    for copy in copies:
        copy.start()
    return copies


def own_quarter():
    return lax.rem(lax.axis_index(TP[0]), 2)


def quarters_of(half):
    own = pl.multiple_of(own_quarter() * QUARTER, 8)
    far = pl.multiple_of((1 - own_quarter()) * QUARTER, 8)
    return half.at[:, pl.ds(own, QUARTER)], half.at[:, pl.ds(far, QUARTER)]


def tiles_to_send(
    far_value_weight,
    far_out_weight,
    far_value_basis,
    far_out_basis,
    weights,
    bases,
    out_weight,
    value_basis,
    out_basis,
    sems,
):
    rows = far_value_weight.shape[0]
    copies = fetched(
        (
            (far_value_basis, value_basis),
            (far_out_basis, out_basis),
            (far_out_weight, out_weight),
            (far_value_weight, weights.at[pl.ds(0, rows)]),
        ),
        sems,
    )
    for copy in copies:
        copy.wait()
    weights[32:48, :] = out_weight[:, :LANES]
    weights[48:64, :] = out_weight[:, LANES:]
    lower = jnp.concatenate([value_basis[:, :LANES], out_basis[:, :LANES]], axis=0)
    upper = jnp.concatenate([value_basis[:, LANES:], out_basis[:, LANES:]], axis=0)
    core = lax.axis_index(CORE)
    half = jnp.where(core == 0, lower.astype(F32), upper.astype(F32))
    mine = jnp.where(own_quarter() == 0, half[:QUARTER], half[QUARTER:]).astype(BF16)
    bases[...] = jnp.broadcast_to(mine[None], bases.shape)


def both_rows(basis):
    return basis[:, :32, :].reshape(-1, LANES), basis[:, 32:, :].reshape(-1, LANES)


def projected(half, out_rows, out_grad, value_rows, value_grad, parts):
    def part(grad, rows):
        count = grad.shape[0]
        both = jnp.concatenate(parts_of(grad[...], 2), axis=0)
        sums = jnp.dot(both, rows, preferred_element_type=F32)
        return sums[:count] + sums[count:]

    peers = parts.shape[0] // 2
    rows = pl.ds(half * peers, peers)
    shape = (peers, LANES // peers, -1)
    parts[rows, :, LANES:] = part(out_grad, out_rows).T.reshape(shape)
    parts[rows, :, :LANES] = part(value_grad(), value_rows).T.reshape(shape)


def own_half(far_own, far_beside, far_value_grad, out_grad, parts, value_grad, basis, sems):
    own, beside = quarters_of(basis)
    *begun, grad_begun = fetched(
        ((far_own, own), (far_beside, beside), (far_value_grad, value_grad)), sems
    )

    def value_grad_now():
        grad_begun.wait()
        return value_grad

    for copy in begun:
        copy.wait()
    value_rows, out_rows = both_rows(basis)
    projected(lax.axis_index(CORE), out_rows, out_grad, value_rows, value_grad_now, parts)


def other_half(own, beside, value_grad, out_grad, begun, parts, basis):
    for at in range(2):

        @pl.when(own_quarter() == at)
        def _(at=at):
            basis[:, at * QUARTER : (at + 1) * QUARTER, :] = own[...]
            basis[:, (1 - at) * QUARTER : (2 - at) * QUARTER, :] = beside[...]

    value_rows, out_rows = both_rows(basis)
    half = 1 - lax.axis_index(CORE)
    projected(half, out_rows, out_grad, value_rows, lambda: value_grad, parts)


def directions(
    arrived,
    value_first,
    value_second,
    out_first,
    out_second,
    value_first_new,
    value_second_new,
    out_first_new,
    out_second_new,
    sent,
):
    total = jnp.sum(arrived[...], axis=0)

    def moments(projected, first, second, first_new, second_new):
        first_now = first_decay * first[...] + (1.0 - first_decay) * projected
        second_now = second_decay * second[...] + (1.0 - second_decay) * projected * projected
        first_new[...] = first_now
        second_new[...] = second_now
        return first_now / jnp.sqrt(second_now)

    value_dir = moments(
        total[:, :LANES], value_first, value_second, value_first_new, value_second_new
    )
    out_dir = moments(total[:, LANES:], out_first, out_second, out_first_new, out_second_new)
    both = jnp.concatenate([value_dir, out_dir], axis=1)
    sent[...] = jnp.broadcast_to(both[None], sent.shape)


def squares(dirs, sums):
    rows = jnp.sum(dirs[...] * dirs[...], axis=0)
    sums[...] = jnp.full(sums.shape, jnp.sum(rows), F32)


def raw_steps(
    far_own,
    far_beside,
    far_other,
    far_diagonal,
    dirs,
    far_value_raw,
    far_out_raw,
    bases,
    value_raw,
    out_raw,
    sems,
):
    targets = quarters_of(bases.at[0]) + quarters_of(bases.at[1])
    copies = fetched(zip((far_own, far_beside, far_other, far_diagonal), targets), sems)
    core = lax.axis_index(CORE)
    peers = dirs.shape[0] // 2
    rows = jnp.concatenate(
        [
            dirs[pl.ds(core * peers, peers)].reshape(LANES, -1),
            dirs[pl.ds((1 - core) * peers, peers)].reshape(LANES, -1),
        ],
        axis=0,
    )

    def stepped(basis, cut):
        cols = cut.shape[1]
        sums = jnp.dot(
            basis, jnp.concatenate(parts_of(cut, 3), axis=1), preferred_element_type=F32
        )
        return sums[:, :cols] + sums[:, cols : 2 * cols] + sums[:, 2 * cols :]

    for copy in copies:
        copy.wait()
    value_basis, out_basis = (
        jnp.concatenate(halves, axis=1) for halves in zip(*(both_rows(bases[at]) for at in (0, 1)))
    )
    value_raw[...] = stepped(value_basis, rows[:, :LANES]).reshape(value_raw.shape)
    sent = fetched(((value_raw, far_value_raw),), sems, 4)
    out_raw[...] = stepped(out_basis, rows[:, LANES:]).reshape(out_raw.shape)
    for copy in sent + fetched(((out_raw, far_out_raw),), sems, 5):
        copy.wait()


CHUNKS = 4


def updates(
    sums,
    value_weight,
    out_weight,
    far_value_raw,
    far_out_raw,
    far_weights,
    value_new,
    out_new,
    value_step,
    out_step,
    far_value_copy,
    far_out_copy,
    weights,
    value_raw,
    out_raw,
    value_copy,
    out_copy,
    sems,
):
    peers = far_weights.shape[0] // CHUNKS
    chunks = [pl.ds(at * peers, peers) for at in range(CHUNKS)]
    arriving = [
        fetched(
            [
                (far.at[chunk], local.at[chunk])
                for far, local in (
                    (far_weights, weights),
                    (far_value_raw, value_raw),
                    (far_out_raw, out_raw),
                )
            ],
            sems,
            3 * at,
        )
        for at, chunk in enumerate(chunks)
    ]
    total = jnp.sum(sums[:, 0, :], axis=0, keepdims=True)
    scale = step_rate / jnp.sqrt(1.0 + total / (R * (W + D)))
    wide = jnp.concatenate([scale, scale], axis=1)
    leaving = []
    for at, chunk in enumerate(chunks):
        for copy in arriving[at]:
            copy.wait()
        step = scale[None] * value_raw[chunk]
        value_copy[chunk] = (weights[chunk, :32, :] - step).astype(BF16)
        step = wide[None] * out_raw[chunk]
        out_copy[chunk, :, :LANES] = (weights[chunk, 32:48, :] - step[:, :, :LANES]).astype(BF16)
        out_copy[chunk, :, LANES:] = (weights[chunk, 48:, :] - step[:, :, LANES:]).astype(BF16)
        leaving += fetched(
            (
                (value_copy.at[chunk], far_value_copy.at[chunk]),
                (out_copy.at[chunk], far_out_copy.at[chunk]),
            ),
            sems,
            3 * CHUNKS + 2 * at,
        )
    shard = lax.axis_index(FS)
    value_now = scale * value_raw[shard]
    out_now = wide * out_raw[shard]
    value_step[...] = value_now
    out_step[...] = out_now
    value_new[...] = value_weight[...] - value_now
    out_new[...] = out_weight[...] - out_now
    for copy in leaving:
        copy.wait()


def beside_pairs():
    def partner(x, core):
        ahead = x % 2 == core
        return (x + (1 if ahead else -1)) % 4

    return [
        ((chip * 4 + x) * 2 + core, (chip * 4 + partner(x, core)) * 2 + core)
        for chip in range(64)
        for x in range(4)
        for core in range(2)
    ]


def sent_across(x, axis):
    return lax.all_to_all(x, axis, 0, 0, tiled=True)


def local(
    layer_input,
    value_cotangent,
    mixed_output,
    output_cotangent,
    value_weight,
    out_weight,
    value_basis,
    out_basis,
    value_first,
    value_second,
    out_first,
    out_second,
):
    peers = lax.axis_size(FS)
    semaphores = pltpu.SemaphoreType.DMA
    weight_tile, basis_tiles = run(
        tiles_to_send,
        [near((64, LANES), F32), far((peers, QUARTER, LANES), BF16)],
        value_weight,
        out_weight,
        value_basis,
        out_basis,
        hbm=(0, 1, 2, 3),
        scratch_shapes=[
            pltpu.VMEM(out_weight.shape, F32),
            pltpu.VMEM(value_basis.shape, BF16),
            pltpu.VMEM(out_basis.shape, BF16),
            semaphores((4,)),
        ],
    )
    weights = lax.all_gather(weight_tile[None], FS, axis=0, tiled=True)

    def grad(cotangent, source):
        return lax.dot_general(
            cotangent, source, (((0,), (0,)), ((), ())), preferred_element_type=F32
        )

    own, value_grad, out_grad = lax.optimization_barrier(
        (
            sent_across(basis_tiles, FS),
            grad(value_cotangent, layer_input),
            grad(output_cotangent, mixed_output),
        )
    )
    beside = lax.ppermute(own, ALL, beside_pairs())
    swap = [(0, 1), (1, 0)]
    other = lax.ppermute(own, CORE, swap)
    diagonal = lax.ppermute(beside, CORE, swap)
    parts = near((peers, R // peers, 3 * LANES), F32)
    half = pltpu.VMEM((peers, 2 * QUARTER, LANES), BF16)
    begun, value_grad = run(
        own_half,
        [parts, near(value_grad.shape, F32)],
        own,
        beside,
        value_grad,
        out_grad,
        flops=10**10,
        hbm=(0, 1, 2),
        scratch_shapes=[half, semaphores((3,))],
    )
    (whole,) = run(
        other_half,
        [parts],
        other,
        diagonal,
        value_grad,
        out_grad,
        begun,
        input_output_aliases={4: 0},
        scratch_shapes=[half],
    )
    arrived = sent_across(whole, FS)
    moment = [far(value_first.shape, F32)] * 2 + [far(out_first.shape, F32)] * 2
    *new_moments, sent = run(
        directions,
        [*moment, parts],
        arrived,
        value_first,
        value_second,
        out_first,
        out_second,
    )
    dirs = sent_across(sent, FS)
    (sums,) = run(squares, [near((8, 1, LANES), F32)], dirs)
    all_sums = sent_across(sums, TP)
    value_whole, out_whole = (peers, 32, LANES), (peers, 16, 2 * LANES)
    value_raw, out_raw = run(
        raw_steps,
        [pltpu.HBM(value_whole, F32), pltpu.HBM(out_whole, F32)],
        own,
        beside,
        other,
        diagonal,
        dirs,
        flops=10**9,
        hbm=(0, 1, 2, 3),
        hbm_outs=(0, 1),
        scratch_shapes=[
            pltpu.VMEM((2, peers, 2 * QUARTER, LANES), BF16),
            pltpu.VMEM(value_whole, F32),
            pltpu.VMEM(out_whole, F32),
            semaphores((6,)),
        ],
    )
    *rows, value_copy, out_copy = run(
        updates,
        [
            far(value_weight.shape, F32),
            far(out_weight.shape, F32),
            far(value_weight.shape, F32),
            far(out_weight.shape, F32),
            far(value_whole, BF16),
            far(out_whole, BF16),
        ],
        all_sums,
        value_weight,
        out_weight,
        value_raw,
        out_raw,
        weights,
        hbm=(3, 4, 5),
        hbm_outs=(4, 5),
        scratch_shapes=[
            pltpu.VMEM(weights.shape, F32),
            pltpu.VMEM(value_whole, F32),
            pltpu.VMEM(out_whole, F32),
            pltpu.VMEM(value_whole, BF16),
            pltpu.VMEM(out_whole, BF16),
            semaphores((5 * CHUNKS,)),
        ],
    )
    return (
        *rows,
        value_copy.reshape(-1, LANES),
        out_copy.reshape(-1, 2 * LANES),
        *new_moments,
    )


def solution(mesh):
    torus = Mesh(mesh.devices.reshape(8, 8, 4, 2), ("fs_0", "fs_1", "tp_0", "tp_1"))
    rows = P(FS, None)
    tile = P(FS, TP)
    return jax.shard_map(
        local,
        mesh=torus,
        in_specs=(rows, tile, rows, tile, tile, tile, rows, rows, tile, tile, tile, tile),
        out_specs=(tile, tile, tile, tile, P(None, TP), P(None, TP), tile, tile, tile, tile),
        check_vma=False,
    )
```

```python
import jax
import jax.numpy as jnp
from jax import lax
from jax.experimental import pallas as pl
from jax.experimental.pallas import tpu as pltpu
from jax.sharding import Mesh
from jax.sharding import PartitionSpec as P


D = 2048
W = 1024
R = 256
FS = ("fs_0", "fs_1")
TP = ("tp_0", "tp_1")
CORE = "tp_1"
ALL = FS + TP
QUARTER = 24
LANES = 128

first_decay = 0.8
second_decay = 0.9
step_rate = 0.1

F32 = jnp.float32
BF16 = jnp.bfloat16


def near(shape, dtype):
    return pltpu.VMEM(shape, dtype)


def far(shape, dtype):
    return jax.ShapeDtypeStruct(shape, dtype)


def run(kernel, outs, *args, flops=0, hbm=(), hbm_outs=(), **options):
    def spec(whether):
        return pl.BlockSpec(memory_space=pltpu.HBM if whether else pltpu.VMEM)

    return pl.pallas_call(
        kernel,
        out_shape=outs,
        in_specs=[spec(at in hbm) for at in range(len(args))],
        out_specs=[spec(at in hbm_outs) for at in range(len(outs))],
        name=kernel.__name__,
        compiler_params=pltpu.CompilerParams(vmem_limit_bytes=16 << 20),
        cost_estimate=pl.CostEstimate(flops=flops, bytes_accessed=1 << 20, transcendentals=0),
        **options,
    )(
        *(
            pltpu.with_memory_space_constraint(x, pltpu.HBM if at in hbm else pltpu.VMEM)
            for at, x in enumerate(args)
        )
    )


def parts_of(wide, count):
    parts = []
    for _ in range(count):
        part = wide.astype(BF16)
        parts.append(part)
        wide = wide - part.astype(F32)
    return parts


def fetched(pairs, sems, first=0):
    copies = [pltpu.make_async_copy(a, b, sems.at[first + at]) for at, (a, b) in enumerate(pairs)]
    for copy in copies:
        copy.start()
    return copies


def own_quarter():
    return lax.rem(lax.axis_index(TP[0]), 2)


def quarters_of(half):
    own = pl.multiple_of(own_quarter() * QUARTER, 8)
    far = pl.multiple_of((1 - own_quarter()) * QUARTER, 8)
    return half.at[:, pl.ds(own, QUARTER)], half.at[:, pl.ds(far, QUARTER)]


def tiles_to_send(
    far_value_weight,
    far_out_weight,
    far_value_basis,
    far_out_basis,
    weights,
    bases,
    out_weight,
    value_basis,
    out_basis,
    sems,
):
    rows = far_value_weight.shape[0]
    copies = fetched(
        (
            (far_value_basis, value_basis),
            (far_out_basis, out_basis),
            (far_out_weight, out_weight),
            (far_value_weight, weights.at[pl.ds(0, rows)]),
        ),
        sems,
    )
    for copy in copies:
        copy.wait()
    weights[32:48, :] = out_weight[:, :LANES]
    weights[48:64, :] = out_weight[:, LANES:]
    lower = jnp.concatenate([value_basis[:, :LANES], out_basis[:, :LANES]], axis=0)
    upper = jnp.concatenate([value_basis[:, LANES:], out_basis[:, LANES:]], axis=0)
    core = lax.axis_index(CORE)
    half = jnp.where(core == 0, lower.astype(F32), upper.astype(F32))
    mine = jnp.where(own_quarter() == 0, half[:QUARTER], half[QUARTER:]).astype(BF16)
    bases[...] = jnp.broadcast_to(mine[None], bases.shape)


def both_rows(basis):
    return basis[:, :32, :].reshape(-1, LANES), basis[:, 32:, :].reshape(-1, LANES)


def staged(far_own, far_value_grad, out_grad, own, value_parts, out_parts, value_grad, sems):
    copies = fetched(((far_own, own), (far_value_grad, value_grad)), sems)
    out_parts[...] = jnp.concatenate(parts_of(out_grad[...], 2), axis=0)
    for copy in copies:
        copy.wait()
    value_parts[...] = jnp.concatenate(parts_of(value_grad[...], 2), axis=0)


def projected(half, own, beside, value_parts, out_parts, parts, basis):
    for at in range(2):

        @pl.when(own_quarter() == at)
        def _(at=at):
            basis[:, at * QUARTER : (at + 1) * QUARTER, :] = own[...]
            basis[:, (1 - at) * QUARTER : (2 - at) * QUARTER, :] = beside[...]

    def part(both, rows):
        count = both.shape[0] // 2
        sums = jnp.dot(both[...], rows, preferred_element_type=F32)
        return sums[:count] + sums[count:]

    value_rows, out_rows = both_rows(basis)
    flipped = jnp.concatenate([part(value_parts, value_rows), part(out_parts, out_rows)], axis=0)
    peers = parts.shape[0] // 2
    parts[pl.ds(half * peers, peers)] = flipped.T.reshape(peers, LANES // peers, -1)


def own_half(own, beside, value_parts, out_parts, parts, basis):
    core = lax.axis_index(CORE)
    projected(core, own, beside, value_parts, out_parts, parts, basis)


def other_half(own, beside, value_parts, out_parts, begun, parts, basis):
    core = lax.axis_index(CORE)
    projected(1 - core, own, beside, value_parts, out_parts, parts, basis)


def directions(
    arrived,
    value_first,
    value_second,
    out_first,
    out_second,
    value_first_new,
    value_second_new,
    out_first_new,
    out_second_new,
    sent,
):
    total = jnp.sum(arrived[...], axis=0)

    def moments(projected, first, second, first_new, second_new):
        first_now = first_decay * first[...] + (1.0 - first_decay) * projected
        second_now = second_decay * second[...] + (1.0 - second_decay) * projected * projected
        first_new[...] = first_now
        second_new[...] = second_now
        return first_now / jnp.sqrt(second_now)

    value_dir = moments(
        total[:, :LANES], value_first, value_second, value_first_new, value_second_new
    )
    out_dir = moments(total[:, LANES:], out_first, out_second, out_first_new, out_second_new)
    both = jnp.concatenate([value_dir, out_dir], axis=1)
    sent[...] = jnp.broadcast_to(both[None], sent.shape)


def squares(dirs, sums):
    rows = jnp.sum(dirs[...] * dirs[...], axis=0)
    sums[...] = jnp.full(sums.shape, jnp.sum(rows), F32)


def raw_steps(
    far_own,
    far_beside,
    far_other,
    far_diagonal,
    dirs,
    far_value_raw,
    far_out_raw,
    bases,
    value_raw,
    out_raw,
    sems,
):
    targets = quarters_of(bases.at[0]) + quarters_of(bases.at[1])
    copies = fetched(zip((far_own, far_beside, far_other, far_diagonal), targets), sems)
    core = lax.axis_index(CORE)
    peers = dirs.shape[0] // 2
    rows = jnp.concatenate(
        [
            dirs[pl.ds(core * peers, peers)].reshape(LANES, -1),
            dirs[pl.ds((1 - core) * peers, peers)].reshape(LANES, -1),
        ],
        axis=0,
    )

    def stepped(basis, cut):
        cols = cut.shape[1]
        sums = jnp.dot(
            basis, jnp.concatenate(parts_of(cut, 3), axis=1), preferred_element_type=F32
        )
        return sums[:, :cols] + sums[:, cols : 2 * cols] + sums[:, 2 * cols :]

    for copy in copies:
        copy.wait()
    value_basis, out_basis = (
        jnp.concatenate(halves, axis=1) for halves in zip(*(both_rows(bases[at]) for at in (0, 1)))
    )
    value_raw[...] = stepped(value_basis, rows[:, :LANES]).reshape(value_raw.shape)
    sent = fetched(((value_raw, far_value_raw),), sems, 4)
    out_raw[...] = stepped(out_basis, rows[:, LANES:]).reshape(out_raw.shape)
    for copy in sent + fetched(((out_raw, far_out_raw),), sems, 5):
        copy.wait()


CHUNKS = 4


def updates(
    sums,
    value_weight,
    out_weight,
    far_value_raw,
    far_out_raw,
    far_weights,
    value_new,
    out_new,
    value_step,
    out_step,
    far_value_copy,
    far_out_copy,
    weights,
    value_raw,
    out_raw,
    value_copy,
    out_copy,
    sems,
):
    peers = far_weights.shape[0] // CHUNKS
    chunks = [pl.ds(at * peers, peers) for at in range(CHUNKS)]
    arriving = [
        fetched(
            [
                (far.at[chunk], local.at[chunk])
                for far, local in (
                    (far_weights, weights),
                    (far_value_raw, value_raw),
                    (far_out_raw, out_raw),
                )
            ],
            sems,
            3 * at,
        )
        for at, chunk in enumerate(chunks)
    ]
    total = jnp.sum(sums[:, 0, :], axis=0, keepdims=True)
    scale = step_rate / jnp.sqrt(1.0 + total / (R * (W + D)))
    wide = jnp.concatenate([scale, scale], axis=1)
    leaving = []
    for at, chunk in enumerate(chunks):
        for copy in arriving[at]:
            copy.wait()
        step = scale[None] * value_raw[chunk]
        value_copy[chunk] = (weights[chunk, :32, :] - step).astype(BF16)
        step = wide[None] * out_raw[chunk]
        out_copy[chunk, :, :LANES] = (weights[chunk, 32:48, :] - step[:, :, :LANES]).astype(BF16)
        out_copy[chunk, :, LANES:] = (weights[chunk, 48:, :] - step[:, :, LANES:]).astype(BF16)
        leaving += fetched(
            (
                (value_copy.at[chunk], far_value_copy.at[chunk]),
                (out_copy.at[chunk], far_out_copy.at[chunk]),
            ),
            sems,
            3 * CHUNKS + 2 * at,
        )
    shard = lax.axis_index(FS)
    value_now = scale * value_raw[shard]
    out_now = wide * out_raw[shard]
    value_step[...] = value_now
    out_step[...] = out_now
    value_new[...] = value_weight[...] - value_now
    out_new[...] = out_weight[...] - out_now
    for copy in leaving:
        copy.wait()


def beside_pairs():
    def partner(x, core):
        ahead = x % 2 == core
        return (x + (1 if ahead else -1)) % 4

    return [
        ((chip * 4 + x) * 2 + core, (chip * 4 + partner(x, core)) * 2 + core)
        for chip in range(64)
        for x in range(4)
        for core in range(2)
    ]


def sent_across(x, axis):
    return lax.all_to_all(x, axis, 0, 0, tiled=True)


def local(
    layer_input,
    value_cotangent,
    mixed_output,
    output_cotangent,
    value_weight,
    out_weight,
    value_basis,
    out_basis,
    value_first,
    value_second,
    out_first,
    out_second,
):
    peers = lax.axis_size(FS)
    semaphores = pltpu.SemaphoreType.DMA
    weight_tile, basis_tiles = run(
        tiles_to_send,
        [near((64, LANES), F32), far((peers, QUARTER, LANES), BF16)],
        value_weight,
        out_weight,
        value_basis,
        out_basis,
        hbm=(0, 1, 2, 3),
        scratch_shapes=[
            pltpu.VMEM(out_weight.shape, F32),
            pltpu.VMEM(value_basis.shape, BF16),
            pltpu.VMEM(out_basis.shape, BF16),
            semaphores((4,)),
        ],
    )
    weights = lax.all_gather(weight_tile[None], FS, axis=0, tiled=True)

    def grad(cotangent, source):
        return lax.dot_general(
            cotangent, source, (((0,), (0,)), ((), ())), preferred_element_type=F32
        )

    own, value_grad, out_grad = lax.optimization_barrier(
        (
            sent_across(basis_tiles, FS),
            grad(value_cotangent, layer_input),
            grad(output_cotangent, mixed_output),
        )
    )
    beside = lax.ppermute(own, ALL, beside_pairs())
    swap = [(0, 1), (1, 0)]
    other = lax.ppermute(own, CORE, swap)
    parts = near((peers, R // peers, 3 * LANES), F32)
    half = pltpu.VMEM((peers, 2 * QUARTER, LANES), BF16)
    own_near, value_parts, out_parts = run(
        staged,
        [
            near(own.shape, BF16),
            near((2 * LANES, value_grad.shape[1]), BF16),
            near((4 * LANES, out_grad.shape[1]), BF16),
        ],
        own,
        value_grad,
        out_grad,
        flops=10**7,
        hbm=(0, 1),
        scratch_shapes=[pltpu.VMEM(value_grad.shape, F32), semaphores((2,))],
    )
    beside, own_near, value_parts, out_parts = lax.optimization_barrier(
        (beside, own_near, value_parts, out_parts)
    )
    diagonal = lax.ppermute(beside, CORE, swap)
    (begun,) = run(
        own_half,
        [parts],
        own_near,
        beside,
        value_parts,
        out_parts,
        flops=10**9,
        scratch_shapes=[half],
    )
    (whole,) = run(
        other_half,
        [parts],
        other,
        diagonal,
        value_parts,
        out_parts,
        begun,
        input_output_aliases={4: 0},
        scratch_shapes=[half],
    )
    arrived = sent_across(whole, FS)
    moment = [far(value_first.shape, F32)] * 2 + [far(out_first.shape, F32)] * 2
    *new_moments, sent = run(
        directions,
        [*moment, parts],
        arrived,
        value_first,
        value_second,
        out_first,
        out_second,
    )
    dirs = sent_across(sent, FS)
    (sums,) = run(squares, [near((8, 1, LANES), F32)], dirs)
    all_sums = sent_across(sums, TP)
    value_whole, out_whole = (peers, 32, LANES), (peers, 16, 2 * LANES)
    value_raw, out_raw = run(
        raw_steps,
        [pltpu.HBM(value_whole, F32), pltpu.HBM(out_whole, F32)],
        own,
        beside,
        other,
        diagonal,
        dirs,
        flops=10**9,
        hbm=(0, 1, 2, 3),
        hbm_outs=(0, 1),
        scratch_shapes=[
            pltpu.VMEM((2, peers, 2 * QUARTER, LANES), BF16),
            pltpu.VMEM(value_whole, F32),
            pltpu.VMEM(out_whole, F32),
            semaphores((6,)),
        ],
    )
    *rows, value_copy, out_copy = run(
        updates,
        [
            far(value_weight.shape, F32),
            far(out_weight.shape, F32),
            far(value_weight.shape, F32),
            far(out_weight.shape, F32),
            far(value_whole, BF16),
            far(out_whole, BF16),
        ],
        all_sums,
        value_weight,
        out_weight,
        value_raw,
        out_raw,
        weights,
        hbm=(3, 4, 5),
        hbm_outs=(4, 5),
        scratch_shapes=[
            pltpu.VMEM(weights.shape, F32),
            pltpu.VMEM(value_whole, F32),
            pltpu.VMEM(out_whole, F32),
            pltpu.VMEM(value_whole, BF16),
            pltpu.VMEM(out_whole, BF16),
            semaphores((5 * CHUNKS,)),
        ],
    )
    return (
        *rows,
        value_copy.reshape(-1, LANES),
        out_copy.reshape(-1, 2 * LANES),
        *new_moments,
    )


def solution(mesh):
    torus = Mesh(mesh.devices.reshape(8, 8, 4, 2), ("fs_0", "fs_1", "tp_0", "tp_1"))
    rows = P(FS, None)
    tile = P(FS, TP)
    return jax.shard_map(
        local,
        mesh=torus,
        in_specs=(rows, tile, rows, tile, tile, tile, rows, rows, tile, tile, tile, tile),
        out_specs=(tile, tile, tile, tile, P(None, TP), P(None, TP), tile, tile, tile, tile),
        check_vma=False,
    )
```

```python
import jax
import jax.numpy as jnp
from jax import lax
from jax.experimental import pallas as pl
from jax.experimental.pallas import tpu as pltpu
from jax.sharding import Mesh
from jax.sharding import PartitionSpec as P


D = 2048
W = 1024
R = 256
FS = ("fs_0", "fs_1")
TP = ("tp_0", "tp_1")
CORE = "tp_1"
ALL = FS + TP
QUARTER = 24
LANES = 128

first_decay = 0.8
second_decay = 0.9
step_rate = 0.1

F32 = jnp.float32
BF16 = jnp.bfloat16


def near(shape, dtype):
    return pltpu.VMEM(shape, dtype)


def far(shape, dtype):
    return jax.ShapeDtypeStruct(shape, dtype)


def run(kernel, outs, *args, flops=0, hbm=(), hbm_outs=(), **options):
    def spec(whether):
        return pl.BlockSpec(memory_space=pltpu.HBM if whether else pltpu.VMEM)

    return pl.pallas_call(
        kernel,
        out_shape=outs,
        in_specs=[spec(at in hbm) for at in range(len(args))],
        out_specs=[spec(at in hbm_outs) for at in range(len(outs))],
        name=kernel.__name__,
        compiler_params=pltpu.CompilerParams(vmem_limit_bytes=16 << 20),
        cost_estimate=pl.CostEstimate(flops=flops, bytes_accessed=1 << 20, transcendentals=0),
        **options,
    )(
        *(
            pltpu.with_memory_space_constraint(x, pltpu.HBM if at in hbm else pltpu.VMEM)
            for at, x in enumerate(args)
        )
    )


def parts_of(wide, count):
    parts = []
    for _ in range(count):
        part = wide.astype(BF16)
        parts.append(part)
        wide = wide - part.astype(F32)
    return parts


def fetched(pairs, sems, first=0):
    copies = [pltpu.make_async_copy(a, b, sems.at[first + at]) for at, (a, b) in enumerate(pairs)]
    for copy in copies:
        copy.start()
    return copies


def own_quarter():
    return lax.rem(lax.axis_index(TP[0]), 2)


def quarters_of(half):
    own = pl.multiple_of(own_quarter() * QUARTER, 8)
    far = pl.multiple_of((1 - own_quarter()) * QUARTER, 8)
    return half.at[:, pl.ds(own, QUARTER)], half.at[:, pl.ds(far, QUARTER)]


def tiles_to_send(
    far_value_weight,
    far_out_weight,
    far_value_basis,
    far_out_basis,
    weights,
    bases,
    out_weight,
    value_basis,
    out_basis,
    sems,
):
    rows = far_value_weight.shape[0]
    copies = fetched(
        (
            (far_value_basis, value_basis),
            (far_out_basis, out_basis),
            (far_out_weight, out_weight),
            (far_value_weight, weights.at[pl.ds(0, rows)]),
        ),
        sems,
    )
    for copy in copies:
        copy.wait()
    weights[32:48, :] = out_weight[:, :LANES]
    weights[48:64, :] = out_weight[:, LANES:]
    lower = jnp.concatenate([value_basis[:, :LANES], out_basis[:, :LANES]], axis=0)
    upper = jnp.concatenate([value_basis[:, LANES:], out_basis[:, LANES:]], axis=0)
    core = lax.axis_index(CORE)
    half = jnp.where(core == 0, lower.astype(F32), upper.astype(F32))
    mine = jnp.where(own_quarter() == 0, half[:QUARTER], half[QUARTER:]).astype(BF16)
    bases[...] = jnp.broadcast_to(mine[None], bases.shape)


def both_rows(basis):
    return basis[:, :32, :].reshape(-1, LANES), basis[:, 32:, :].reshape(-1, LANES)


def staged(far_own, far_value_grad, out_grad, own, value_parts, out_parts, value_grad, sems):
    copies = fetched(((far_own, own), (far_value_grad, value_grad)), sems)
    out_parts[...] = jnp.concatenate(parts_of(out_grad[...], 2), axis=0)
    for copy in copies:
        copy.wait()
    value_parts[...] = jnp.concatenate(parts_of(value_grad[...], 2), axis=0)


def projected(half, own, beside, value_parts, out_parts, parts, basis):
    for at in range(2):

        @pl.when(own_quarter() == at)
        def _(at=at):
            basis[:, at * QUARTER : (at + 1) * QUARTER, :] = own[...]
            basis[:, (1 - at) * QUARTER : (2 - at) * QUARTER, :] = beside[...]

    def part(both, rows):
        count = both.shape[0] // 2
        sums = jnp.dot(both[...], rows, preferred_element_type=F32)
        return sums[:count] + sums[count:]

    value_rows, out_rows = both_rows(basis)
    flipped = jnp.concatenate([part(value_parts, value_rows), part(out_parts, out_rows)], axis=0)
    peers = parts.shape[0] // 2
    parts[pl.ds(half * peers, peers)] = flipped.T.reshape(peers, LANES // peers, -1)


def own_half(own, beside, value_parts, out_parts, parts, basis):
    core = lax.axis_index(CORE)
    projected(core, own, beside, value_parts, out_parts, parts, basis)


def other_half(own, beside, value_parts, out_parts, begun, parts, basis):
    core = lax.axis_index(CORE)
    projected(1 - core, own, beside, value_parts, out_parts, parts, basis)


def directions(
    arrived,
    value_first,
    value_second,
    out_first,
    out_second,
    value_first_new,
    value_second_new,
    out_first_new,
    out_second_new,
    sent,
):
    total = jnp.sum(arrived[...], axis=0)

    def moments(projected, first, second, first_new, second_new):
        first_now = first_decay * first[...] + (1.0 - first_decay) * projected
        second_now = second_decay * second[...] + (1.0 - second_decay) * projected * projected
        first_new[...] = first_now
        second_new[...] = second_now
        return first_now / jnp.sqrt(second_now)

    value_dir = moments(
        total[:, :LANES], value_first, value_second, value_first_new, value_second_new
    )
    out_dir = moments(total[:, LANES:], out_first, out_second, out_first_new, out_second_new)
    both = jnp.concatenate([value_dir, out_dir], axis=1)
    sent[...] = jnp.broadcast_to(both[None], sent.shape)


def squares(dirs, sums):
    rows = jnp.sum(dirs[...] * dirs[...], axis=0)
    sums[...] = jnp.full(sums.shape, jnp.sum(rows), F32)


def raw_steps(
    far_own,
    far_beside,
    far_other,
    far_diagonal,
    dirs,
    value_raw,
    far_out_raw,
    bases,
    out_raw,
    sems,
):
    targets = quarters_of(bases.at[0]) + quarters_of(bases.at[1])
    copies = fetched(zip((far_own, far_beside, far_other, far_diagonal), targets), sems)
    core = lax.axis_index(CORE)
    peers = dirs.shape[0] // 2
    rows = jnp.concatenate(
        [
            dirs[pl.ds(core * peers, peers)].reshape(LANES, -1),
            dirs[pl.ds((1 - core) * peers, peers)].reshape(LANES, -1),
        ],
        axis=0,
    )

    def stepped(basis, cut):
        cols = cut.shape[1]
        sums = jnp.dot(
            basis, jnp.concatenate(parts_of(cut, 3), axis=1), preferred_element_type=F32
        )
        return sums[:, :cols] + sums[:, cols : 2 * cols] + sums[:, 2 * cols :]

    for copy in copies:
        copy.wait()
    value_basis, out_basis = (
        jnp.concatenate(halves, axis=1) for halves in zip(*(both_rows(bases[at]) for at in (0, 1)))
    )
    out_raw[...] = stepped(out_basis, rows[:, LANES:]).reshape(out_raw.shape)
    sent = fetched(((out_raw, far_out_raw),), sems, 4)
    value_raw[...] = stepped(value_basis, rows[:, :LANES]).reshape(value_raw.shape)
    for copy in sent:
        copy.wait()


CHUNKS = 4


def updates(
    sums,
    value_raw,
    far_out_raw,
    far_value_weight,
    far_out_weight,
    far_weights,
    far_value_new,
    far_out_new,
    far_value_step,
    far_out_step,
    far_value_copy,
    far_out_copy,
    value_weight,
    out_weight,
    out_now,
    weights,
    out_raw,
    value_new,
    out_new,
    value_step,
    out_step,
    value_copy,
    out_copy,
    sems,
):
    shard = lax.axis_index(FS)
    own_rows = fetched(
        (
            (far_value_weight, value_weight),
            (far_out_weight, out_weight),
            (far_out_raw.at[shard], out_now),
        ),
        sems,
    )
    peers = far_weights.shape[0] // CHUNKS
    chunks = [pl.ds(at * peers, peers) for at in range(CHUNKS)]
    arriving = [
        fetched(
            (
                (far_weights.at[chunk], weights.at[chunk]),
                (far_out_raw.at[chunk], out_raw.at[chunk]),
            ),
            sems,
            3 + 2 * at,
        )
        for at, chunk in enumerate(chunks)
    ]
    total = jnp.sum(sums[:, 0, :], axis=0, keepdims=True)
    scale = step_rate / jnp.sqrt(1.0 + total / (R * (W + D)))
    wide = jnp.concatenate([scale, scale], axis=1)
    for copy in own_rows:
        copy.wait()
    value_step[...] = scale * value_raw[shard]
    out_step[...] = wide * out_now[...]
    value_new[...] = value_weight[...] - value_step[...]
    out_new[...] = out_weight[...] - out_step[...]
    leaving = fetched(
        (
            (value_new, far_value_new),
            (out_new, far_out_new),
            (value_step, far_value_step),
            (out_step, far_out_step),
        ),
        sems,
        3 + 2 * CHUNKS,
    )
    for at, chunk in enumerate(chunks):
        for copy in arriving[at]:
            copy.wait()
        step = scale[None] * value_raw[chunk]
        value_copy[chunk] = (weights[chunk, :32, :] - step).astype(BF16)
        step = wide[None] * out_raw[chunk]
        out_copy[chunk, :, :LANES] = (weights[chunk, 32:48, :] - step[:, :, :LANES]).astype(BF16)
        out_copy[chunk, :, LANES:] = (weights[chunk, 48:, :] - step[:, :, LANES:]).astype(BF16)
        leaving += fetched(
            (
                (value_copy.at[chunk], far_value_copy.at[chunk]),
                (out_copy.at[chunk], far_out_copy.at[chunk]),
            ),
            sems,
            7 + 2 * CHUNKS + 2 * at,
        )
    for copy in leaving:
        copy.wait()


def beside_pairs():
    def partner(x, core):
        ahead = x % 2 == core
        return (x + (1 if ahead else -1)) % 4

    return [
        ((chip * 4 + x) * 2 + core, (chip * 4 + partner(x, core)) * 2 + core)
        for chip in range(64)
        for x in range(4)
        for core in range(2)
    ]


def sent_across(x, axis):
    return lax.all_to_all(x, axis, 0, 0, tiled=True)


def local(
    layer_input,
    value_cotangent,
    mixed_output,
    output_cotangent,
    value_weight,
    out_weight,
    value_basis,
    out_basis,
    value_first,
    value_second,
    out_first,
    out_second,
):
    peers = lax.axis_size(FS)
    semaphores = pltpu.SemaphoreType.DMA
    weight_tile, basis_tiles = run(
        tiles_to_send,
        [near((64, LANES), F32), far((peers, QUARTER, LANES), BF16)],
        value_weight,
        out_weight,
        value_basis,
        out_basis,
        hbm=(0, 1, 2, 3),
        scratch_shapes=[
            pltpu.VMEM(out_weight.shape, F32),
            pltpu.VMEM(value_basis.shape, BF16),
            pltpu.VMEM(out_basis.shape, BF16),
            semaphores((4,)),
        ],
    )
    weights = lax.all_gather(weight_tile[None], FS, axis=0, tiled=True)

    def grad(cotangent, source):
        return lax.dot_general(
            cotangent, source, (((0,), (0,)), ((), ())), preferred_element_type=F32
        )

    own, value_grad, out_grad = lax.optimization_barrier(
        (
            sent_across(basis_tiles, FS),
            grad(value_cotangent, layer_input),
            grad(output_cotangent, mixed_output),
        )
    )
    beside = lax.ppermute(own, ALL, beside_pairs())
    swap = [(0, 1), (1, 0)]
    other = lax.ppermute(own, CORE, swap)
    parts = near((peers, R // peers, 3 * LANES), F32)
    half = pltpu.VMEM((peers, 2 * QUARTER, LANES), BF16)
    own_near, value_parts, out_parts = run(
        staged,
        [
            near(own.shape, BF16),
            near((2 * LANES, value_grad.shape[1]), BF16),
            near((4 * LANES, out_grad.shape[1]), BF16),
        ],
        own,
        value_grad,
        out_grad,
        flops=10**7,
        hbm=(0, 1),
        scratch_shapes=[pltpu.VMEM(value_grad.shape, F32), semaphores((2,))],
    )
    beside, own_near, value_parts, out_parts = lax.optimization_barrier(
        (beside, own_near, value_parts, out_parts)
    )
    diagonal = lax.ppermute(beside, CORE, swap)
    (begun,) = run(
        own_half,
        [parts],
        own_near,
        beside,
        value_parts,
        out_parts,
        flops=10**9,
        scratch_shapes=[half],
    )
    (whole,) = run(
        other_half,
        [parts],
        other,
        diagonal,
        value_parts,
        out_parts,
        begun,
        input_output_aliases={4: 0},
        scratch_shapes=[half],
    )
    arrived = sent_across(whole, FS)
    moment = [far(value_first.shape, F32)] * 2 + [far(out_first.shape, F32)] * 2
    *new_moments, sent = run(
        directions,
        [*moment, parts],
        arrived,
        value_first,
        value_second,
        out_first,
        out_second,
    )
    dirs = sent_across(sent, FS)
    (sums,) = run(squares, [near((8, 1, LANES), F32)], dirs)
    all_sums = sent_across(sums, TP)
    value_whole, out_whole = (peers, 32, LANES), (peers, 16, 2 * LANES)
    value_raw, out_raw = run(
        raw_steps,
        [near(value_whole, F32), pltpu.HBM(out_whole, F32)],
        own,
        beside,
        other,
        diagonal,
        dirs,
        flops=10**9,
        hbm=(0, 1, 2, 3),
        hbm_outs=(1,),
        scratch_shapes=[
            pltpu.VMEM((2, peers, 2 * QUARTER, LANES), BF16),
            pltpu.VMEM(out_whole, F32),
            semaphores((5,)),
        ],
    )
    tiles = (value_weight.shape, out_weight.shape) * 2
    *rows, value_copy, out_copy = run(
        updates,
        [*(far(tile, F32) for tile in tiles), far(value_whole, BF16), far(out_whole, BF16)],
        all_sums,
        value_raw,
        out_raw,
        value_weight,
        out_weight,
        weights,
        hbm=(2, 3, 4, 5),
        hbm_outs=range(6),
        scratch_shapes=[
            *(pltpu.VMEM(tile, F32) for tile in tiles[:2]),
            pltpu.VMEM(tiles[1], F32),
            pltpu.VMEM(weights.shape, F32),
            pltpu.VMEM(out_whole, F32),
            *(pltpu.VMEM(tile, F32) for tile in tiles),
            pltpu.VMEM(value_whole, BF16),
            pltpu.VMEM(out_whole, BF16),
            semaphores((4 * CHUNKS + 7,)),
        ],
    )
    return (
        *rows,
        value_copy.reshape(-1, LANES),
        out_copy.reshape(-1, 2 * LANES),
        *new_moments,
    )


def solution(mesh):
    torus = Mesh(mesh.devices.reshape(8, 8, 4, 2), ("fs_0", "fs_1", "tp_0", "tp_1"))
    rows = P(FS, None)
    tile = P(FS, TP)
    return jax.shard_map(
        local,
        mesh=torus,
        in_specs=(rows, tile, rows, tile, tile, tile, rows, rows, tile, tile, tile, tile),
        out_specs=(tile, tile, tile, tile, P(None, TP), P(None, TP), tile, tile, tile, tile),
        check_vma=False,
    )
```

```python
import jax
import jax.numpy as jnp
from jax import lax
from jax.experimental import pallas as pl
from jax.experimental.pallas import tpu as pltpu
from jax.sharding import Mesh
from jax.sharding import PartitionSpec as P


D = 2048
W = 1024
R = 256
FS = ("fs_0", "fs_1")
TP = ("tp_0", "tp_1")
CORE = "tp_1"
ALL = FS + TP
QUARTER = 24
LANES = 128

first_decay = 0.8
second_decay = 0.9
step_rate = 0.1

F32 = jnp.float32
BF16 = jnp.bfloat16


def near(shape, dtype):
    return pltpu.VMEM(shape, dtype)


def far(shape, dtype):
    return jax.ShapeDtypeStruct(shape, dtype)


def run(kernel, outs, *args, flops=0, hbm=(), hbm_outs=(), **options):
    def spec(whether):
        return pl.BlockSpec(memory_space=pltpu.HBM if whether else pltpu.VMEM)

    return pl.pallas_call(
        kernel,
        out_shape=outs,
        in_specs=[spec(at in hbm) for at in range(len(args))],
        out_specs=[spec(at in hbm_outs) for at in range(len(outs))],
        name=kernel.__name__,
        compiler_params=pltpu.CompilerParams(vmem_limit_bytes=16 << 20),
        cost_estimate=pl.CostEstimate(flops=flops, bytes_accessed=1 << 20, transcendentals=0),
        **options,
    )(
        *(
            pltpu.with_memory_space_constraint(x, pltpu.HBM if at in hbm else pltpu.VMEM)
            for at, x in enumerate(args)
        )
    )


def parts_of(wide, count):
    parts = []
    for _ in range(count):
        part = wide.astype(BF16)
        parts.append(part)
        wide = wide - part.astype(F32)
    return parts


def fetched(pairs, sems, first=0):
    copies = [pltpu.make_async_copy(a, b, sems.at[first + at]) for at, (a, b) in enumerate(pairs)]
    for copy in copies:
        copy.start()
    return copies


def own_quarter():
    return lax.rem(lax.axis_index(TP[0]), 2)


def quarters_of(half):
    own = pl.multiple_of(own_quarter() * QUARTER, 8)
    far = pl.multiple_of((1 - own_quarter()) * QUARTER, 8)
    return half.at[:, pl.ds(own, QUARTER)], half.at[:, pl.ds(far, QUARTER)]


def tiles_to_send(
    far_value_weight,
    far_out_weight,
    far_value_basis,
    far_out_basis,
    weights,
    far_bases,
    out_weight,
    value_basis,
    out_basis,
    bases,
    sems,
):
    rows = far_value_weight.shape[0]
    *copies, weight_copy, out_copy = fetched(
        (
            (far_value_basis, value_basis),
            (far_out_basis, out_basis),
            (far_value_weight, weights.at[pl.ds(0, rows)]),
            (far_out_weight, out_weight),
        ),
        sems,
    )
    for copy in copies:
        copy.wait()
    lower = jnp.concatenate([value_basis[:, :LANES], out_basis[:, :LANES]], axis=0)
    upper = jnp.concatenate([value_basis[:, LANES:], out_basis[:, LANES:]], axis=0)
    core = lax.axis_index(CORE)
    half = jnp.where(core == 0, lower.astype(F32), upper.astype(F32))
    mine = jnp.where(own_quarter() == 0, half[:QUARTER], half[QUARTER:]).astype(BF16)
    bases[...] = jnp.broadcast_to(mine[None], bases.shape)
    (leaving,) = fetched(((bases, far_bases),), sems, 4)
    out_copy.wait()
    weights[32:48, :] = out_weight[:, :LANES]
    weights[48:64, :] = out_weight[:, LANES:]
    weight_copy.wait()
    leaving.wait()


def both_rows(basis):
    return basis[:, :32, :].reshape(-1, LANES), basis[:, 32:, :].reshape(-1, LANES)


def staged(far_own, far_value_grad, out_grad, own, value_parts, out_parts, value_grad, sems):
    copies = fetched(((far_own, own), (far_value_grad, value_grad)), sems)
    out_parts[...] = jnp.concatenate(parts_of(out_grad[...], 2), axis=0)
    for copy in copies:
        copy.wait()
    value_parts[...] = jnp.concatenate(parts_of(value_grad[...], 2), axis=0)


def projected(half, own, beside, value_parts, out_parts, parts, basis):
    for at in range(2):

        @pl.when(own_quarter() == at)
        def _(at=at):
            basis[:, at * QUARTER : (at + 1) * QUARTER, :] = own[...]
            basis[:, (1 - at) * QUARTER : (2 - at) * QUARTER, :] = beside[...]

    def part(both, rows):
        count = both.shape[0] // 2
        sums = jnp.dot(both[...], rows, preferred_element_type=F32)
        return sums[:count] + sums[count:]

    value_rows, out_rows = both_rows(basis)
    flipped = jnp.concatenate([part(value_parts, value_rows), part(out_parts, out_rows)], axis=0)
    peers = parts.shape[0] // 2
    parts[pl.ds(half * peers, peers)] = flipped.T.reshape(peers, LANES // peers, -1)


def own_half(own, beside, value_parts, out_parts, parts, basis):
    core = lax.axis_index(CORE)
    projected(core, own, beside, value_parts, out_parts, parts, basis)


def other_half(own, beside, value_parts, out_parts, begun, parts, basis):
    core = lax.axis_index(CORE)
    projected(1 - core, own, beside, value_parts, out_parts, parts, basis)


def directions(
    arrived,
    value_first,
    value_second,
    out_first,
    out_second,
    value_first_new,
    value_second_new,
    out_first_new,
    out_second_new,
    sent,
):
    total = jnp.sum(arrived[...], axis=0)

    def moments(projected, first, second, first_new, second_new):
        first_now = first_decay * first[...] + (1.0 - first_decay) * projected
        second_now = second_decay * second[...] + (1.0 - second_decay) * projected * projected
        first_new[...] = first_now
        second_new[...] = second_now
        return first_now / jnp.sqrt(second_now)

    value_dir = moments(
        total[:, :LANES], value_first, value_second, value_first_new, value_second_new
    )
    out_dir = moments(total[:, LANES:], out_first, out_second, out_first_new, out_second_new)
    both = jnp.concatenate([value_dir, out_dir], axis=1)
    sent[...] = jnp.broadcast_to(both[None], sent.shape)


def squares(dirs, sums):
    rows = jnp.sum(dirs[...] * dirs[...], axis=0)
    sums[...] = jnp.full(sums.shape, jnp.sum(rows), F32)


def raw_steps(
    far_own,
    far_beside,
    far_other,
    far_diagonal,
    dirs,
    value_raw,
    far_out_raw,
    bases,
    out_raw,
    sems,
):
    targets = quarters_of(bases.at[0]) + quarters_of(bases.at[1])
    copies = fetched(zip((far_own, far_beside, far_other, far_diagonal), targets), sems)
    core = lax.axis_index(CORE)
    peers = dirs.shape[0] // 2
    rows = jnp.concatenate(
        [
            dirs[pl.ds(core * peers, peers)].reshape(LANES, -1),
            dirs[pl.ds((1 - core) * peers, peers)].reshape(LANES, -1),
        ],
        axis=0,
    )

    def stepped(basis, cut):
        cols = cut.shape[1]
        sums = jnp.dot(
            basis, jnp.concatenate(parts_of(cut, 3), axis=1), preferred_element_type=F32
        )
        return sums[:, :cols] + sums[:, cols : 2 * cols] + sums[:, 2 * cols :]

    for copy in copies:
        copy.wait()
    value_basis, out_basis = (
        jnp.concatenate(halves, axis=1) for halves in zip(*(both_rows(bases[at]) for at in (0, 1)))
    )
    out_raw[...] = stepped(out_basis, rows[:, LANES:]).reshape(out_raw.shape)
    sent = fetched(((out_raw, far_out_raw),), sems, 4)
    value_raw[...] = stepped(value_basis, rows[:, :LANES]).reshape(value_raw.shape)
    for copy in sent:
        copy.wait()


CHUNKS = 8


def updates(
    sums,
    value_raw,
    far_out_raw,
    far_value_weight,
    far_out_weight,
    far_weights,
    far_value_new,
    far_out_new,
    far_value_step,
    far_out_step,
    far_value_copy,
    far_out_copy,
    value_weight,
    out_weight,
    out_now,
    weights,
    out_raw,
    value_new,
    out_new,
    value_step,
    out_step,
    value_copy,
    out_copy,
    sems,
):
    shard = lax.axis_index(FS)
    own_rows = fetched(
        (
            (far_value_weight, value_weight),
            (far_out_weight, out_weight),
            (far_out_raw.at[shard], out_now),
        ),
        sems,
    )
    peers = far_weights.shape[0] // CHUNKS
    chunks = [pl.ds(at * peers, peers) for at in range(CHUNKS)]
    arriving = [
        fetched(
            (
                (far_weights.at[chunk], weights.at[chunk]),
                (far_out_raw.at[chunk], out_raw.at[chunk]),
            ),
            sems,
            3 + 2 * at,
        )
        for at, chunk in enumerate(chunks)
    ]
    total = jnp.sum(sums[:, 0, :], axis=0, keepdims=True)
    scale = step_rate / jnp.sqrt(1.0 + total / (R * (W + D)))
    wide = jnp.concatenate([scale, scale], axis=1)
    for copy in own_rows:
        copy.wait()
    value_step[...] = scale * value_raw[shard]
    out_step[...] = wide * out_now[...]
    value_new[...] = value_weight[...] - value_step[...]
    out_new[...] = out_weight[...] - out_step[...]
    leaving = fetched(
        (
            (value_new, far_value_new),
            (out_new, far_out_new),
            (value_step, far_value_step),
            (out_step, far_out_step),
        ),
        sems,
        3 + 2 * CHUNKS,
    )
    for at, chunk in enumerate(chunks):
        for copy in arriving[at]:
            copy.wait()
        step = scale[None] * value_raw[chunk]
        value_copy[chunk] = (weights[chunk, :32, :] - step).astype(BF16)
        step = wide[None] * out_raw[chunk]
        out_copy[chunk, :, :LANES] = (weights[chunk, 32:48, :] - step[:, :, :LANES]).astype(BF16)
        out_copy[chunk, :, LANES:] = (weights[chunk, 48:, :] - step[:, :, LANES:]).astype(BF16)
        leaving += fetched(
            (
                (value_copy.at[chunk], far_value_copy.at[chunk]),
                (out_copy.at[chunk], far_out_copy.at[chunk]),
            ),
            sems,
            7 + 2 * CHUNKS + 2 * at,
        )
    for copy in leaving:
        copy.wait()


def beside_pairs():
    def partner(x, core):
        ahead = x % 2 == core
        return (x + (1 if ahead else -1)) % 4

    return [
        ((chip * 4 + x) * 2 + core, (chip * 4 + partner(x, core)) * 2 + core)
        for chip in range(64)
        for x in range(4)
        for core in range(2)
    ]


def sent_across(x, axis):
    return lax.all_to_all(x, axis, 0, 0, tiled=True)


def local(
    layer_input,
    value_cotangent,
    mixed_output,
    output_cotangent,
    value_weight,
    out_weight,
    value_basis,
    out_basis,
    value_first,
    value_second,
    out_first,
    out_second,
):
    peers = lax.axis_size(FS)
    semaphores = pltpu.SemaphoreType.DMA
    weight_tile, basis_tiles = run(
        tiles_to_send,
        [near((64, LANES), F32), pltpu.HBM((peers, QUARTER, LANES), BF16)],
        value_weight,
        out_weight,
        value_basis,
        out_basis,
        hbm=(0, 1, 2, 3),
        scratch_shapes=[
            pltpu.VMEM(out_weight.shape, F32),
            pltpu.VMEM(value_basis.shape, BF16),
            pltpu.VMEM(out_basis.shape, BF16),
            pltpu.VMEM((peers, QUARTER, LANES), BF16),
            semaphores((5,)),
        ],
        hbm_outs=(1,),
    )
    weights = lax.all_gather(weight_tile[None], FS, axis=0, tiled=True)

    def grad(cotangent, source):
        return lax.dot_general(
            cotangent, source, (((0,), (0,)), ((), ())), preferred_element_type=F32
        )

    own, value_grad, out_grad = lax.optimization_barrier(
        (
            sent_across(basis_tiles, FS),
            grad(value_cotangent, layer_input),
            grad(output_cotangent, mixed_output),
        )
    )
    beside = lax.ppermute(own, ALL, beside_pairs())
    swap = [(0, 1), (1, 0)]
    other = lax.ppermute(own, CORE, swap)
    parts = near((peers, R // peers, 3 * LANES), F32)
    half = pltpu.VMEM((peers, 2 * QUARTER, LANES), BF16)
    own_near, value_parts, out_parts = run(
        staged,
        [
            near(own.shape, BF16),
            near((2 * LANES, value_grad.shape[1]), BF16),
            near((4 * LANES, out_grad.shape[1]), BF16),
        ],
        own,
        value_grad,
        out_grad,
        flops=10**7,
        hbm=(0, 1),
        scratch_shapes=[pltpu.VMEM(value_grad.shape, F32), semaphores((2,))],
    )
    beside, own_near, value_parts, out_parts = lax.optimization_barrier(
        (beside, own_near, value_parts, out_parts)
    )
    diagonal = lax.ppermute(beside, CORE, swap)
    (begun,) = run(
        own_half,
        [parts],
        own_near,
        beside,
        value_parts,
        out_parts,
        flops=10**9,
        scratch_shapes=[half],
    )
    (whole,) = run(
        other_half,
        [parts],
        other,
        diagonal,
        value_parts,
        out_parts,
        begun,
        input_output_aliases={4: 0},
        scratch_shapes=[half],
    )
    arrived = sent_across(whole, FS)
    moment = [far(value_first.shape, F32)] * 2 + [far(out_first.shape, F32)] * 2
    *new_moments, sent = run(
        directions,
        [*moment, parts],
        arrived,
        value_first,
        value_second,
        out_first,
        out_second,
    )
    dirs = sent_across(sent, FS)
    (sums,) = run(squares, [near((8, 1, LANES), F32)], dirs)
    all_sums = sent_across(sums, TP)
    value_whole, out_whole = (peers, 32, LANES), (peers, 16, 2 * LANES)
    value_raw, out_raw = run(
        raw_steps,
        [near(value_whole, F32), pltpu.HBM(out_whole, F32)],
        own,
        beside,
        other,
        diagonal,
        dirs,
        flops=10**9,
        hbm=(0, 1, 2, 3),
        hbm_outs=(1,),
        scratch_shapes=[
            pltpu.VMEM((2, peers, 2 * QUARTER, LANES), BF16),
            pltpu.VMEM(out_whole, F32),
            semaphores((5,)),
        ],
    )
    tiles = (value_weight.shape, out_weight.shape) * 2
    *rows, value_copy, out_copy = run(
        updates,
        [*(far(tile, F32) for tile in tiles), far(value_whole, BF16), far(out_whole, BF16)],
        all_sums,
        value_raw,
        out_raw,
        value_weight,
        out_weight,
        weights,
        hbm=(2, 3, 4, 5),
        hbm_outs=range(6),
        scratch_shapes=[
            *(pltpu.VMEM(tile, F32) for tile in tiles[:2]),
            pltpu.VMEM(tiles[1], F32),
            pltpu.VMEM(weights.shape, F32),
            pltpu.VMEM(out_whole, F32),
            *(pltpu.VMEM(tile, F32) for tile in tiles),
            pltpu.VMEM(value_whole, BF16),
            pltpu.VMEM(out_whole, BF16),
            semaphores((4 * CHUNKS + 7,)),
        ],
    )
    return (
        *rows,
        value_copy.reshape(-1, LANES),
        out_copy.reshape(-1, 2 * LANES),
        *new_moments,
    )


def solution(mesh):
    torus = Mesh(mesh.devices.reshape(8, 8, 4, 2), ("fs_0", "fs_1", "tp_0", "tp_1"))
    rows = P(FS, None)
    tile = P(FS, TP)
    return jax.shard_map(
        local,
        mesh=torus,
        in_specs=(rows, tile, rows, tile, tile, tile, rows, rows, tile, tile, tile, tile),
        out_specs=(tile, tile, tile, tile, P(None, TP), P(None, TP), tile, tile, tile, tile),
        check_vma=False,
    )
```

```python
import jax
import jax.numpy as jnp
from jax import lax
from jax.experimental import pallas as pl
from jax.experimental.pallas import tpu as pltpu
from jax.sharding import Mesh
from jax.sharding import PartitionSpec as P


D = 2048
W = 1024
R = 256
FS = ("fs_0", "fs_1")
TP = ("tp_0", "tp_1")
CORE = "tp_1"
BASIS_ROWS = 48
LANES = 128

first_decay = 0.8
second_decay = 0.9
step_rate = 0.1

F32 = jnp.float32
BF16 = jnp.bfloat16


def near(shape, dtype):
    return pltpu.VMEM(shape, dtype)


def far(shape, dtype):
    return jax.ShapeDtypeStruct(shape, dtype)


def run(kernel, outs, *args, flops=0, hbm=(), hbm_outs=(), **options):
    def spec(whether):
        return pl.BlockSpec(memory_space=pltpu.HBM if whether else pltpu.VMEM)

    return pl.pallas_call(
        kernel,
        out_shape=outs,
        in_specs=[spec(at in hbm) for at in range(len(args))],
        out_specs=[spec(at in hbm_outs) for at in range(len(outs))],
        name=kernel.__name__,
        compiler_params=pltpu.CompilerParams(vmem_limit_bytes=16 << 20),
        cost_estimate=pl.CostEstimate(flops=flops, bytes_accessed=1 << 20, transcendentals=0),
        **options,
    )(
        *(
            pltpu.with_memory_space_constraint(x, pltpu.HBM if at in hbm else pltpu.VMEM)
            for at, x in enumerate(args)
        )
    )


def parts_of(wide, count):
    parts = []
    for _ in range(count):
        part = wide.astype(BF16)
        parts.append(part)
        wide = wide - part.astype(F32)
    return parts


def fetched(pairs, sems, first=0):
    copies = [pltpu.make_async_copy(a, b, sems.at[first + at]) for at, (a, b) in enumerate(pairs)]
    for copy in copies:
        copy.start()
    return copies


def tiles_to_send(
    far_value_weight,
    far_out_weight,
    far_value_basis,
    far_out_basis,
    weights,
    bases,
    out_weight,
    value_basis,
    out_basis,
    sems,
):
    rows = far_value_weight.shape[0]
    copies = fetched(
        (
            (far_value_basis, value_basis),
            (far_out_basis, out_basis),
            (far_out_weight, out_weight),
            (far_value_weight, weights.at[pl.ds(0, rows)]),
        ),
        sems,
    )
    for copy in copies:
        copy.wait()
    weights[32:48, :] = out_weight[:, :LANES]
    weights[48:64, :] = out_weight[:, LANES:]
    lower = jnp.concatenate([value_basis[:, :LANES], out_basis[:, :LANES]], axis=0)
    upper = jnp.concatenate([value_basis[:, LANES:], out_basis[:, LANES:]], axis=0)
    core = lax.axis_index(CORE)
    mine = jnp.where(core == 0, lower.astype(F32), upper.astype(F32)).astype(BF16)
    bases[...] = jnp.broadcast_to(mine[None], bases.shape)


def both_rows(basis):
    return basis[:, :32, :].reshape(-1, LANES), basis[:, 32:, :].reshape(-1, LANES)


def staged(far_own, far_value_grad, out_grad, own, value_parts, out_parts, value_grad, sems):
    copies = fetched(((far_own, own), (far_value_grad, value_grad)), sems)
    out_parts[...] = jnp.concatenate(parts_of(out_grad[...], 2), axis=0)
    for copy in copies:
        copy.wait()
    value_parts[...] = jnp.concatenate(parts_of(value_grad[...], 2), axis=0)


def projected(half, basis, value_parts, out_parts, parts):
    def part(both, rows):
        count = both.shape[0] // 2
        sums = jnp.dot(both[...], rows, preferred_element_type=F32)
        return sums[:count] + sums[count:]

    value_rows, out_rows = both_rows(basis)
    flipped = jnp.concatenate([part(value_parts, value_rows), part(out_parts, out_rows)], axis=0)
    peers = parts.shape[0] // 2
    parts[pl.ds(half * peers, peers)] = flipped.T.reshape(peers, LANES // peers, -1)


def own_half(own, value_parts, out_parts, parts):
    projected(lax.axis_index(CORE), own, value_parts, out_parts, parts)


def other_half(other, value_parts, out_parts, begun, parts):
    projected(1 - lax.axis_index(CORE), other, value_parts, out_parts, parts)


def directions(
    arrived,
    value_first,
    value_second,
    out_first,
    out_second,
    value_first_new,
    value_second_new,
    out_first_new,
    out_second_new,
    sent,
):
    total = jnp.sum(arrived[...], axis=0)

    def moments(projected, first, second, first_new, second_new):
        first_now = first_decay * first[...] + (1.0 - first_decay) * projected
        second_now = second_decay * second[...] + (1.0 - second_decay) * projected * projected
        first_new[...] = first_now
        second_new[...] = second_now
        return first_now / jnp.sqrt(second_now)

    value_dir = moments(
        total[:, :LANES], value_first, value_second, value_first_new, value_second_new
    )
    out_dir = moments(total[:, LANES:], out_first, out_second, out_first_new, out_second_new)
    both = jnp.concatenate([value_dir, out_dir], axis=1)
    sent[...] = jnp.broadcast_to(both[None], sent.shape)


def squares(dirs, sums):
    rows = jnp.sum(dirs[...] * dirs[...], axis=0)
    sums[...] = jnp.full(sums.shape, jnp.sum(rows), F32)


def raw_steps(
    far_own,
    far_other,
    dirs,
    value_raw,
    far_out_raw,
    bases,
    out_raw,
    sems,
):
    copies = fetched(((far_own, bases.at[0]), (far_other, bases.at[1])), sems)
    core = lax.axis_index(CORE)
    peers = dirs.shape[0] // 2
    rows = jnp.concatenate(
        [
            dirs[pl.ds(core * peers, peers)].reshape(LANES, -1),
            dirs[pl.ds((1 - core) * peers, peers)].reshape(LANES, -1),
        ],
        axis=0,
    )

    def stepped(basis, cut):
        cols = cut.shape[1]
        sums = jnp.dot(
            basis, jnp.concatenate(parts_of(cut, 3), axis=1), preferred_element_type=F32
        )
        return sums[:, :cols] + sums[:, cols : 2 * cols] + sums[:, 2 * cols :]

    for copy in copies:
        copy.wait()
    value_basis, out_basis = (
        jnp.concatenate(halves, axis=1) for halves in zip(*(both_rows(bases[at]) for at in (0, 1)))
    )
    out_raw[...] = stepped(out_basis, rows[:, LANES:]).reshape(out_raw.shape)
    sent = fetched(((out_raw, far_out_raw),), sems, 2)
    value_raw[...] = stepped(value_basis, rows[:, :LANES]).reshape(value_raw.shape)
    for copy in sent:
        copy.wait()


CHUNKS = 4


def updates(
    sums,
    value_raw,
    far_out_raw,
    far_value_weight,
    far_out_weight,
    far_weights,
    far_value_new,
    far_out_new,
    far_value_step,
    far_out_step,
    far_value_copy,
    far_out_copy,
    value_weight,
    out_weight,
    out_now,
    weights,
    out_raw,
    value_new,
    out_new,
    value_step,
    out_step,
    value_copy,
    out_copy,
    sems,
):
    shard = lax.axis_index(FS)
    own_rows = fetched(
        (
            (far_value_weight, value_weight),
            (far_out_weight, out_weight),
            (far_out_raw.at[shard], out_now),
        ),
        sems,
    )
    peers = far_weights.shape[0] // CHUNKS
    chunks = [pl.ds(at * peers, peers) for at in range(CHUNKS)]
    arriving = [
        fetched(
            (
                (far_weights.at[chunk], weights.at[chunk]),
                (far_out_raw.at[chunk], out_raw.at[chunk]),
            ),
            sems,
            3 + 2 * at,
        )
        for at, chunk in enumerate(chunks)
    ]
    total = jnp.sum(sums[:, 0, :], axis=0, keepdims=True)
    scale = step_rate / jnp.sqrt(1.0 + total / (R * (W + D)))
    wide = jnp.concatenate([scale, scale], axis=1)
    for copy in own_rows:
        copy.wait()
    value_step[...] = scale * value_raw[shard]
    out_step[...] = wide * out_now[...]
    value_new[...] = value_weight[...] - value_step[...]
    out_new[...] = out_weight[...] - out_step[...]
    leaving = fetched(
        (
            (value_new, far_value_new),
            (out_new, far_out_new),
            (value_step, far_value_step),
            (out_step, far_out_step),
        ),
        sems,
        3 + 2 * CHUNKS,
    )
    for at, chunk in enumerate(chunks):
        for copy in arriving[at]:
            copy.wait()
        step = scale[None] * value_raw[chunk]
        value_copy[chunk] = (weights[chunk, :32, :] - step).astype(BF16)
        step = wide[None] * out_raw[chunk]
        out_copy[chunk, :, :LANES] = (weights[chunk, 32:48, :] - step[:, :, :LANES]).astype(BF16)
        out_copy[chunk, :, LANES:] = (weights[chunk, 48:, :] - step[:, :, LANES:]).astype(BF16)
        leaving += fetched(
            (
                (value_copy.at[chunk], far_value_copy.at[chunk]),
                (out_copy.at[chunk], far_out_copy.at[chunk]),
            ),
            sems,
            7 + 2 * CHUNKS + 2 * at,
        )
    for copy in leaving:
        copy.wait()


def sent_across(x, axis):
    return lax.all_to_all(x, axis, 0, 0, tiled=True)


def local(
    layer_input,
    value_cotangent,
    mixed_output,
    output_cotangent,
    value_weight,
    out_weight,
    value_basis,
    out_basis,
    value_first,
    value_second,
    out_first,
    out_second,
):
    peers = lax.axis_size(FS)
    semaphores = pltpu.SemaphoreType.DMA
    weight_tile, basis_tiles = run(
        tiles_to_send,
        [near((64, LANES), F32), far((peers, BASIS_ROWS, LANES), BF16)],
        value_weight,
        out_weight,
        value_basis,
        out_basis,
        hbm=(0, 1, 2, 3),
        scratch_shapes=[
            pltpu.VMEM(out_weight.shape, F32),
            pltpu.VMEM(value_basis.shape, BF16),
            pltpu.VMEM(out_basis.shape, BF16),
            semaphores((4,)),
        ],
    )
    weights = lax.all_gather(weight_tile[None], FS, axis=0, tiled=True)

    def grad(cotangent, source):
        return lax.dot_general(
            cotangent, source, (((0,), (0,)), ((), ())), preferred_element_type=F32
        )

    own, value_grad, out_grad = lax.optimization_barrier(
        (
            sent_across(basis_tiles, FS),
            grad(value_cotangent, layer_input),
            grad(output_cotangent, mixed_output),
        )
    )
    other = lax.ppermute(own, CORE, [(0, 1), (1, 0)])
    parts = near((peers, R // peers, 3 * LANES), F32)
    own_near, value_parts, out_parts = run(
        staged,
        [
            near(own.shape, BF16),
            near((2 * LANES, value_grad.shape[1]), BF16),
            near((4 * LANES, out_grad.shape[1]), BF16),
        ],
        own,
        value_grad,
        out_grad,
        flops=10**7,
        hbm=(0, 1),
        scratch_shapes=[pltpu.VMEM(value_grad.shape, F32), semaphores((2,))],
    )
    (begun,) = run(own_half, [parts], own_near, value_parts, out_parts, flops=10**10)
    (whole,) = run(
        other_half, [parts], other, value_parts, out_parts, begun, input_output_aliases={3: 0}
    )
    arrived = sent_across(whole, FS)
    moment = [far(value_first.shape, F32)] * 2 + [far(out_first.shape, F32)] * 2
    *new_moments, sent = run(
        directions,
        [*moment, parts],
        arrived,
        value_first,
        value_second,
        out_first,
        out_second,
    )
    dirs = sent_across(sent, FS)
    (sums,) = run(squares, [near((8, 1, LANES), F32)], dirs)
    all_sums = sent_across(sums, TP)
    value_whole, out_whole = (peers, 32, LANES), (peers, 16, 2 * LANES)
    value_raw, out_raw = run(
        raw_steps,
        [near(value_whole, F32), pltpu.HBM(out_whole, F32)],
        own,
        other,
        dirs,
        flops=10**9,
        hbm=(0, 1),
        hbm_outs=(1,),
        scratch_shapes=[
            pltpu.VMEM((2, *own.shape), BF16),
            pltpu.VMEM(out_whole, F32),
            semaphores((3,)),
        ],
    )
    tiles = (value_weight.shape, out_weight.shape) * 2
    *rows, value_copy, out_copy = run(
        updates,
        [*(far(tile, F32) for tile in tiles), far(value_whole, BF16), far(out_whole, BF16)],
        all_sums,
        value_raw,
        out_raw,
        value_weight,
        out_weight,
        weights,
        hbm=(2, 3, 4, 5),
        hbm_outs=range(6),
        scratch_shapes=[
            *(pltpu.VMEM(tile, F32) for tile in tiles[:2]),
            pltpu.VMEM(tiles[1], F32),
            pltpu.VMEM(weights.shape, F32),
            pltpu.VMEM(out_whole, F32),
            *(pltpu.VMEM(tile, F32) for tile in tiles),
            pltpu.VMEM(value_whole, BF16),
            pltpu.VMEM(out_whole, BF16),
            semaphores((4 * CHUNKS + 7,)),
        ],
    )
    return (
        *rows,
        value_copy.reshape(-1, LANES),
        out_copy.reshape(-1, 2 * LANES),
        *new_moments,
    )


def solution(mesh):
    torus = Mesh(mesh.devices.reshape(8, 8, 4, 2), ("fs_0", "fs_1", "tp_0", "tp_1"))
    rows = P(FS, None)
    tile = P(FS, TP)
    return jax.shard_map(
        local,
        mesh=torus,
        in_specs=(rows, tile, rows, tile, tile, tile, rows, rows, tile, tile, tile, tile),
        out_specs=(tile, tile, tile, tile, P(None, TP), P(None, TP), tile, tile, tile, tile),
        check_vma=False,
    )
```
